32 devices in a mesh: sp: 8 (over z, y), dp: 4 (over x, core).
Axes of the slice: x: 2, y: 2, z: 4, core: 2. Of those that a mesh axis runs over, the one named last changes fastest.
Arguments:
- queries: bfloat16 [4, 1024, 2048], P('dp', 'sp'), may hold values from -8 to 8
- keys: bfloat16 [4, 1024, 2048], P('dp', 'sp'), may hold values from -8 to 8
- values: bfloat16 [4, 1024, 2048], P('dp', 'sp'), may hold values from -6 to 6
- proj_weight: bfloat16 [2048, 2048], P('sp'), may hold values from -0.125 to 0.125
- residual: bfloat16 [4, 1024, 2048], P('dp', 'sp'), may hold values from -6 to 6
- norm_gain: float32 [2048], replicated, may hold values from 0.1 to 1.9
- route: int32 [4, 1024, 2], P('dp', 'sp'), may hold values from 0 to 7, all different within a row; in each aligned block of 128 rows (0 to 127, 128 to 255, ..., all dimensions but the last counted through in order) at most 64 rows name the same one
- route_weight: float32 [4, 1024, 2], P('dp', 'sp'), may hold values from 0.1 to 1
- w_gate: bfloat16 [8, 2048, 1024], P('sp'), may hold values from -0.125 to 0.125
- w_up: bfloat16 [8, 2048, 1024], P('sp'), may hold values from -0.125 to 0.125
- w_down: bfloat16 [8, 1024, 2048], P('sp'), may hold values from -0.1875 to 0.1875
Outputs:
- mixed: bfloat16 [4, 1024, 2048], P('dp', 'sp')
The draws below stay inside these ranges and needn't reach their ends.
Inputs may be any that keep to these rules, and one draw needn't show every extreme that they name: `route`: in the rows of one device no expert is named by more than 64 rows, a bound that some block reaches.
All inputs are finite; a program needn't handle non-finite values.
Results may differ from the reference program's by a relative error of at most 0.013.
Values may be sent and summed in bfloat16 or wider, within the bound.
No kernel may reach another device: no remote copies, remote signals or barrier semaphores. Data moves between devices by JAX's collectives and lax.ppermute only.
A program may use at most 128 MiB of HBM per device.

```python
import math
import jax
import jax.numpy as jnp
import numpy as np
from jax import lax

D = 2048
HEADS = 16
HEAD_DIM = 128
FFE = 1024
SEQ_DEV = 128
EXPERTS = 8
LENGTH = 1024
SEQS = 4
CAP = 64
N_SP = 8
N_DP = 4


def head_plan(key):
    first, second, third = jax.random.split(jax.random.fold_in(key, 7), 3)
    direction = jnp.where(jax.random.bernoulli(first, 0.5, (HEADS, HEAD_DIM)), 1.0, -1.0).astype(jnp.float32)
    slow = jax.random.bernoulli(second, 0.5, (HEADS,))
    level = jnp.where(slow, -jnp.log(1.0 * LENGTH) - 1.5, -jnp.log(100.0))
    drift = jax.random.uniform(third, (SEQS, LENGTH // 64, HEADS), jnp.float32, -0.8, 0.8)
    drift = jnp.repeat(drift, 64, axis=1)
    return (direction, level[None, None, :] + drift)


def noise(key):
    sample = jnp.clip(jax.random.normal(key, (SEQS, LENGTH, HEADS, HEAD_DIM), jnp.float32), -6.0, 6.0)
    return sample


def draw_keys(key, part):
    direction, level = head_plan(key)
    sample = noise(jax.random.fold_in(key, 11)) + direction[None, None, :, :]
    return sample.reshape(SEQS, LENGTH, HEADS * HEAD_DIM).astype(jnp.bfloat16)


def draw_queries(key, part):
    direction, level = head_plan(key)
    factor = level / jnp.sqrt(1.0 * HEAD_DIM)
    sample = noise(jax.random.fold_in(key, 13)) + factor[..., None] * direction[None, None, :, :]
    return sample.reshape(SEQS, LENGTH, HEADS * HEAD_DIM).astype(jnp.bfloat16)


def shard_levels(own_key, extent, pieces, low, high):
    gain, own = 1.0, jax.random.fold_in(own_key, 6)
    for dim, blocks in pieces:
        heights = jnp.exp(jax.random.uniform(jax.random.fold_in(own, dim), (blocks,), jnp.float32, low / len(pieces), high / len(pieces)))
        gain = gain * jnp.repeat(heights, extent[dim] // blocks).reshape([-1 if axis == dim else 1 for axis in range(len(extent))])
    return gain


def assign_block(stream_key, own, number, rows, amount, top, most, lean):
    order = jax.random.permutation(stream_key, amount)
    packed, common = portions_of(amount, rows * top, most, lean, True), portions_of(amount, rows * top, most, lean, False)
    places = jnp.arange(amount)

    def named(sizes, offset_by):
        used = int((sizes > 0).sum())
        fixed = max(1, used // 4)
        passed = fixed + (places - fixed + offset_by * (used - fixed)) % max(1, amount - fixed)
        return jnp.zeros((amount,), jnp.int32).at[order[jnp.where(places < fixed, places, passed)]].set(jnp.asarray(sizes, jnp.int32))

    sizes = jnp.where(number % 4 == 0, named(packed, number // 4), named(common, number - number // 4 - 1))
    mixed = jax.random.permutation(jax.random.fold_in(own, 3), amount)
    giver, receiver = mixed[0:amount // 2 * 2:2], mixed[1:amount // 2 * 2:2]
    margin = jnp.minimum(sizes[giver] - 1, most - sizes[receiver]) // 2
    margin = jnp.where((giver == order[0]) | (receiver == order[0]) | (sizes[receiver] == 0), 0, jnp.maximum(margin, 0))
    passed = jax.random.randint(jax.random.fold_in(own, 4), (amount // 2,), 0, 1 << 20) % (margin + 1)
    sizes = sizes.at[giver].add(-passed).at[receiver].add(passed)
    items = jnp.searchsorted(jnp.cumsum(sizes), jnp.arange(rows * top), side="right").astype(jnp.int32)
    grid = items.reshape(top, rows).T
    grid = grid[jax.random.permutation(jax.random.fold_in(own, 1), rows)]
    offset_by = jax.random.randint(jax.random.fold_in(own, 2), (rows, 1), 0, top)
    return jnp.take_along_axis(grid, (jnp.arange(top)[None, :] + offset_by) % top, axis=1)


def portions_of(count, total, reach, skew, full):
    loads = [(1 << 20) // math.isqrt(standing ** skew) + 1 for standing in range(1, count + 1)]
    largest = reach if full else min(reach, max(-(-total // count), total * loads[0] // sum(loads)))
    least = 1 if total - largest >= count - 1 else 0
    holding, surplus = [largest] + [least] * (count - 1), total - largest - least * (count - 1)
    while surplus > 0:
        movable = [i for i in range(1, count) if holding[i] < largest] or [i for i in range(1, count) if holding[i] < reach]
        whole, budget = sum([loads[i] for i in movable]), surplus
        for i in movable:
            extra = min(reach - holding[i], max(1, budget * loads[i] // whole), surplus)
            holding[i] = holding[i] + extra
            surplus = surplus - extra
    return np.array(holding)


def bell_draw(rng, extent, spread, most, shards=(), held_as=jnp.bfloat16):
    drawn = spread * jax.random.normal(rng, extent, jnp.float32)
    if shards:
        drawn = drawn * shard_levels(rng, extent, shards, -0.22, 0.18)
    return jnp.clip(drawn, -most, most).astype(held_as)


def setup_inputs(seed: int = 0) -> dict:
    splits = jax.random.split(jax.random.key(seed), 12)
    queries = draw_queries(jax.random.fold_in(splits[11], 71), 0)
    keys = draw_keys(jax.random.fold_in(splits[11], 71), 0)
    values = bell_draw(splits[2], (SEQS, LENGTH, D), 1.0, 6.0, ((0, 4), (1, 8)))
    proj_weight = bell_draw(splits[3], (D, D), D ** -0.5, 0.125, ((0, 8),))
    residual = bell_draw(splits[4], (SEQS, LENGTH, D), 1.0, 6.0, ((0, 4), (1, 8)))
    norm_gain = jnp.clip(1.0 + 0.18 * jax.random.normal(splits[5], (D,), jnp.float32), 0.1, 1.9)
    route_keys = jax.random.split(jax.random.fold_in(splits[6], 1), SEQS * LENGTH // SEQ_DEV)
    route_turns = jax.random.permutation(jax.random.fold_in(splits[6], 3), SEQS * LENGTH // SEQ_DEV)
    route = jax.vmap(lambda own, number: assign_block(jax.random.fold_in(splits[6], 2), own, number, SEQ_DEV, EXPERTS, 2, CAP, 2))(route_keys, route_turns).reshape((SEQS, LENGTH, 2))
    route_weight = jnp.clip(0.1 + 0.9 * jax.random.uniform(splits[7], (SEQS, LENGTH, 2), jnp.float32) ** shard_levels(splits[7], (SEQS, LENGTH, 2), ((0, 4), (1, 8)), -0.2, 0.2), 0.1, 1.0)
    w_gate = bell_draw(splits[8], (EXPERTS, D, FFE), D ** -0.5, 0.125, ((0, 8),))
    w_up = bell_draw(splits[9], (EXPERTS, D, FFE), D ** -0.5, 0.125, ((0, 8),))
    w_down = bell_draw(splits[10], (EXPERTS, FFE, D), FFE ** -0.5, 0.1875, ((0, 8),))
    return {"queries": queries, "keys": keys, "values": values, "proj_weight": proj_weight, "residual": residual, "norm_gain": norm_gain, "route": route, "route_weight": route_weight, "w_gate": w_gate, "w_up": w_up, "w_down": w_down}


EPS = 1e-06

def one_head(args):
    query, key, value = args
    length = query.shape[0]
    scores = jnp.dot(query, key.T, preferred_element_type=jnp.float32) * HEAD_DIM ** (-0.5)
    position = jnp.arange(length)
    causal = position[None, :] < position[:, None]
    softer = jnp.where(causal, jax.nn.softplus(scores), 0.0)
    suffix = lax.cumsum(softer, axis=1, reverse=True)
    weight = jnp.exp(jnp.where(causal, scores - suffix, -jnp.inf)).astype(jnp.bfloat16)
    return jnp.dot(weight, value, preferred_element_type=jnp.float32).astype(jnp.bfloat16)

def by_heads(array):
    seqs, length, width = array.shape
    heads = width // HEAD_DIM
    return array.reshape(seqs, length, heads, HEAD_DIM).transpose(0, 2, 1, 3).reshape(seqs * heads, length, HEAD_DIM)

def reference(queries, keys, values, proj_weight, residual, norm_gain, route, route_weight, w_gate, w_up, w_down):
    seqs, length, width = queries.shape
    heads = width // HEAD_DIM
    attended = lax.map(one_head, (by_heads(queries), by_heads(keys), by_heads(values)))
    attended = attended.reshape(seqs, heads, length, HEAD_DIM).transpose(0, 2, 1, 3).reshape(seqs * length, width)
    projected = jnp.dot(attended, proj_weight, preferred_element_type=jnp.float32)
    stream = (residual.reshape(seqs * length, width).astype(jnp.float32) + projected).astype(jnp.bfloat16)
    stream_f = stream.astype(jnp.float32)
    normed = (stream_f * lax.rsqrt(lax.optimization_barrier(jnp.mean(stream_f * stream_f, axis=-1, keepdims=True)) + EPS) * norm_gain).astype(jnp.bfloat16)
    flat_route = route.reshape(seqs * length, 2)
    flat_weight = route_weight.reshape(seqs * length, 2)
    bound = CAP * N_SP * N_DP

    def per_expert(total, inputs):
        expert, gate_w, up_w, down_w = inputs
        named = flat_route == expert
        scale = lax.optimization_barrier(jnp.sum(jnp.where(named, flat_weight, 0.0), axis=1))
        used = jnp.any(named, axis=1)
        index = jnp.nonzero(used, size=bound, fill_value=0)[0]
        valid = jnp.arange(bound) < jnp.sum(used.astype(jnp.int32))
        rows = normed[index]
        gate = jnp.dot(rows, gate_w, preferred_element_type=jnp.float32)
        upper = jnp.dot(rows, up_w, preferred_element_type=jnp.float32)
        hidden = (jax.nn.silu(gate) * upper).astype(jnp.bfloat16)
        result = jnp.dot(hidden, down_w, preferred_element_type=jnp.float32).astype(jnp.bfloat16)
        addend = jnp.where(valid[:, None], scale[index][:, None] * result.astype(jnp.float32), 0.0)
        return (total.at[index].add(addend), None)
    experts = w_gate.shape[0]
    total, unused = lax.scan(per_expert, stream.astype(jnp.float32), (jnp.arange(experts).astype(jnp.int32), w_gate, w_up, w_down))
    return total.astype(jnp.bfloat16).reshape(seqs, length, width)
```

```python
import functools

import jax
import jax.numpy as jnp
import numpy as np
from jax import lax
from jax.experimental import pallas as pl
from jax.experimental.pallas import tpu as pltpu
from jax.sharding import PartitionSpec as P

HEADS = 16
EPS = 1e-06


def ring_order(mesh):
    count = mesh.shape["sp"]
    plain = list(range(count))
    try:
        axis = list(mesh.axis_names).index("sp")
        line = np.moveaxis(mesh.devices, axis, 0).reshape(count, -1)[:, 0]
        spots = [tuple(device.coords) for device in line]
    except Exception:
        return plain
    moving = [d for d in range(len(spots[0])) if len({s[d] for s in spots}) > 1]
    if len(moving) != 2:
        return plain
    first, second = sorted(moving, key=lambda d: -len({s[d] for s in spots}))
    where = {(s[first], s[second]): i for i, s in enumerate(spots)}
    rows = sorted({s[first] for s in spots})
    cols = sorted({s[second] for s in spots})
    if len(where) != count or len(rows) * len(cols) != count or len(rows) % 2:
        return plain
    path = []
    for number, row in enumerate(rows):
        inner = cols[1:] if number % 2 == 0 else cols[1:][::-1]
        path.extend((row, col) for col in inner)
    path.extend((row, cols[0]) for row in reversed(rows))
    return [where[spot] for spot in path]


def pack_heads(queries, keys, values, span, heads_here, size):
    rows = queries.shape[0]

    def kernel(q_ref, k_ref, v_ref, *outs):
        for head in range(heads_here):
            cols = slice(head * size, (head + 1) * size)
            for part, ref in enumerate((q_ref, k_ref, v_ref)):
                outs[head][0, :, part * size : (part + 1) * size] = ref[:, cols]

    block = pl.BlockSpec((rows, heads_here * size), lambda d: (0, d))
    return pl.pallas_call(
        kernel,
        grid=(span,),
        in_specs=[block, block, block],
        out_specs=[pl.BlockSpec((1, rows, 3 * size), lambda d: (d, 0, 0))] * heads_here,
        out_shape=[jax.ShapeDtypeStruct((span, rows, 3 * size), queries.dtype)] * heads_here,
        name="pack_heads",
    )(queries, keys, values)


def attend(packed, size):
    length = packed.shape[0]
    block = min(256, length)
    blocks = length // block
    scale = size ** (-0.5)

    def kernel(x_ref, o_ref):
        row = lax.broadcasted_iota(jnp.int32, (block, block), 0)
        col = lax.broadcasted_iota(jnp.int32, (block, block), 1)
        later = (row > col).astype(jnp.bfloat16)
        causal = col < row
        for qb in range(blocks):
            q_rows = slice(qb * block, (qb + 1) * block)
            query = x_ref[q_rows, 0:size]
            carry = jnp.zeros((block, 1), jnp.float32)
            total = jnp.zeros((block, size), jnp.float32)
            for kb in range(qb, -1, -1):
                k_rows = slice(kb * block, (kb + 1) * block)
                score = scale * lax.dot_general(
                    query,
                    x_ref[k_rows, size : 2 * size],
                    (((1,), (1,)), ((), ())),
                    preferred_element_type=jnp.float32,
                )
                soft = jnp.maximum(score, 0.0) + jnp.log(1.0 + jnp.exp(-jnp.abs(score)))
                rest = score - soft
                if kb == qb:
                    soft = jnp.where(causal, soft, 0.0)
                high = soft.astype(jnp.bfloat16)
                low = (soft - high.astype(jnp.float32)).astype(jnp.bfloat16)
                behind = jnp.dot(high, later, preferred_element_type=jnp.float32)
                behind = behind + jnp.dot(low, later, preferred_element_type=jnp.float32)
                weight = jnp.exp(rest - behind - carry)
                if kb == qb:
                    weight = jnp.where(causal, weight, 0.0)
                total = total + jnp.dot(
                    weight.astype(jnp.bfloat16),
                    x_ref[k_rows, 2 * size : 3 * size],
                    preferred_element_type=jnp.float32,
                )
                if kb > 0:
                    carry = carry + behind[:, 0:1] + soft[:, 0:1]
            o_ref[q_rows, :] = total.astype(o_ref.dtype)

    return pl.pallas_call(
        kernel,
        out_shape=jax.ShapeDtypeStruct((length, size), packed.dtype),
        name="attend",
    )(packed)


def expert_pair(first, second, scale, w_gate, w_up, w_down):
    rows, width = first.shape
    hidden_units = w_gate.shape[1]
    chunk = min(256, hidden_units)

    def kernel(a_ref, b_ref, s_ref, g_ref, u_ref, d_ref, oa_ref, ob_ref, x_ref, acc_ref):
        step = pl.program_id(0)

        @pl.when(step == 0)
        def _():
            x_ref[:rows] = a_ref[...]
            x_ref[rows:] = b_ref[...]

        x = x_ref[...]
        gate = jnp.dot(x, g_ref[...], preferred_element_type=jnp.float32)
        upper = jnp.dot(x, u_ref[...], preferred_element_type=jnp.float32)
        hidden = (gate / (1.0 + jnp.exp(-gate)) * upper).astype(jnp.bfloat16)
        part = jnp.dot(hidden, d_ref[...], preferred_element_type=jnp.float32)

        @pl.when(step == 0)
        def _():
            acc_ref[...] = part

        @pl.when(step > 0)
        def _():
            acc_ref[...] += part

        @pl.when(step == pl.num_programs(0) - 1)
        def _():
            out = (acc_ref[...] * s_ref[...]).astype(oa_ref.dtype)
            oa_ref[...] = out[:rows]
            ob_ref[...] = out[rows:]

    whole = pl.BlockSpec((rows, width), lambda i: (0, 0))
    shape = jax.ShapeDtypeStruct((rows, width), first.dtype)
    return pl.pallas_call(
        kernel,
        grid=(hidden_units // chunk,),
        in_specs=[
            whole,
            whole,
            pl.BlockSpec((2 * rows, 1), lambda i: (0, 0)),
            pl.BlockSpec((width, chunk), lambda i: (0, i)),
            pl.BlockSpec((width, chunk), lambda i: (0, i)),
            pl.BlockSpec((chunk, width), lambda i: (i, 0)),
        ],
        out_specs=[whole, whole],
        out_shape=[shape, shape],
        scratch_shapes=[
            pltpu.VMEM((2 * rows, width), first.dtype),
            pltpu.VMEM((2 * rows, width), jnp.float32),
        ],
        cost_estimate=pl.CostEstimate(
            flops=12 * rows * width * hidden_units,
            transcendentals=2 * rows * hidden_units,
            bytes_accessed=6 * width * hidden_units,
        ),
        name="expert_pair",
    )(first, second, scale, w_gate, w_up, w_down)


def body(
    ring,
    queries,
    keys,
    values,
    proj_weight,
    residual,
    norm_gain,
    route,
    route_weight,
    w_gate,
    w_up,
    w_down,
):
    span = lax.axis_size("sp")
    rows, width = queries.shape[1:]
    heads_here = HEADS // span
    size = width // HEADS
    half = rows // 2
    forward = [(ring[i], ring[(i + 1) % span]) for i in range(span)]
    backward = [(b, a) for a, b in forward]
    me = lax.axis_index("sp")
    order = jnp.asarray(np.array(ring, np.int32))
    place = jnp.asarray(np.argsort(np.array(ring)).astype(np.int32))[me]

    def block_at(offset):
        return order[(place + offset) % span]

    named = route[0][None, :, :] == jnp.arange(span, dtype=jnp.int32)[:, None, None]
    scale = jnp.sum(jnp.where(named, route_weight[0][None], 0.0), axis=2)
    scale_all = lax.all_to_all(scale, "sp", split_axis=0, concat_axis=0, tiled=True)

    packed = pack_heads(queries[0], keys[0], values[0], span, heads_here, size)
    heads = []
    for head in packed:
        arrived = lax.all_to_all(head, "sp", split_axis=0, concat_axis=0, tiled=True)
        heads.append(attend(arrived.reshape(span * rows, 3 * size), size))
    attended = jnp.concatenate(heads, axis=1) if heads_here > 1 else heads[0]

    def projected(block, part):
        piece = lax.dynamic_slice_in_dim(attended, block * rows + part * half, half, 0)
        return jnp.dot(piece, proj_weight, preferred_element_type=jnp.float32)

    ahead = projected(block_at(-1), 0).astype(jnp.bfloat16)
    astern = projected(block_at(1), 1).astype(jnp.bfloat16)
    for step in range(1, span):
        ahead = lax.ppermute(ahead, "sp", forward)
        astern = lax.ppermute(astern, "sp", backward)
        if step < span - 1:
            ahead = (ahead + projected(block_at(-1 - step), 0)).astype(jnp.bfloat16)
            astern = (astern + projected(block_at(1 + step), 1)).astype(jnp.bfloat16)

    def finish(got, part):
        own = residual[0][part * half : (part + 1) * half].astype(jnp.float32)
        stream = (own + (got + projected(me, part))).astype(jnp.bfloat16)
        stream_f = stream.astype(jnp.float32)
        normed = (
            stream_f
            * lax.rsqrt(jnp.mean(stream_f * stream_f, axis=-1, keepdims=True) + EPS)
            * norm_gain
        ).astype(jnp.bfloat16)
        return stream_f, normed

    stream_a, norm_a = finish(ahead, 0)
    stream_b, norm_b = finish(astern, 1)

    def expert(first, second, block_first, block_second):
        both = jnp.concatenate([scale_all[block_first, :half], scale_all[block_second, half:]])
        return expert_pair(first, second, both[:, None], w_gate[0], w_up[0], w_down[0])

    own_a, own_b = expert(norm_a, norm_b, me, me)
    sum_a = sum_b = None
    for step in range(1, span):
        norm_a = lax.ppermute(norm_a, "sp", forward)
        norm_b = lax.ppermute(norm_b, "sp", backward)
        out_a, out_b = expert(norm_a, norm_b, block_at(-step), block_at(step))
        if step > 1:
            out_a, out_b = sum_a + out_a, sum_b + out_b
        sum_a = lax.ppermute(out_a, "sp", forward)
        sum_b = lax.ppermute(out_b, "sp", backward)
    mixed = [
        (s + (g.astype(jnp.float32) + o.astype(jnp.float32))).astype(jnp.bfloat16)
        for s, g, o in ((stream_a, sum_a, own_a), (stream_b, sum_b, own_b))
    ]
    return jnp.concatenate(mixed, axis=0)[None]


def solution(mesh):
    rows = P("dp", "sp", None)
    return jax.shard_map(
        functools.partial(body, ring_order(mesh)),
        mesh=mesh,
        in_specs=(
            rows,
            rows,
            rows,
            P("sp", None),
            rows,
            P(),
            rows,
            rows,
            P("sp", None, None),
            P("sp", None, None),
            P("sp", None, None),
        ),
        out_specs=rows,
        check_vma=False,
    )
```

```python
import functools

import jax
import jax.numpy as jnp
import numpy as np
from jax import lax
from jax.experimental import pallas as pl
from jax.experimental.pallas import tpu as pltpu
from jax.sharding import PartitionSpec as P

HEADS = 16
EPS = 1e-06
VMEM_LIMIT = 16 << 20
EXTRA = 128


def ring_order(mesh):
    count = mesh.shape["sp"]
    plain = list(range(count))
    try:
        axis = list(mesh.axis_names).index("sp")
        line = np.moveaxis(mesh.devices, axis, 0).reshape(count, -1)[:, 0]
        spots = [tuple(device.coords) for device in line]
    except Exception:
        return plain
    moving = [d for d in range(len(spots[0])) if len({s[d] for s in spots}) > 1]
    if len(moving) != 2:
        return plain
    first, second = sorted(moving, key=lambda d: -len({s[d] for s in spots}))
    where = {(s[first], s[second]): i for i, s in enumerate(spots)}
    rows = sorted({s[first] for s in spots})
    cols = sorted({s[second] for s in spots})
    if len(where) != count or len(rows) * len(cols) != count or len(rows) % 2:
        return plain
    path = []
    for number, row in enumerate(rows):
        inner = cols[1:] if number % 2 == 0 else cols[1:][::-1]
        path.extend((row, col) for col in inner)
    path.extend((row, cols[0]) for row in reversed(rows))
    return [where[spot] for spot in path]


def pack_heads(targets, queries, keys, values, heads_here, size):
    rows = queries.shape[0]
    span = targets.shape[0]

    def kernel(t_ref, q_ref, k_ref, v_ref, *outs):
        for shift in range(span):
            start = t_ref[shift] * (heads_here * size)
            for head in range(heads_here):
                cols = pl.ds(pl.multiple_of(start + head * size, size), size)
                out = outs[head * span + shift]
                for part, ref in enumerate((q_ref, k_ref, v_ref)):
                    out[:, part * size : (part + 1) * size] = ref[:, cols]

    shape = jax.ShapeDtypeStruct((rows, 3 * size), queries.dtype)
    flat = pl.pallas_call(
        kernel,
        in_specs=[pl.BlockSpec(memory_space=pltpu.SMEM)] + [pl.BlockSpec(memory_space=pltpu.VMEM)] * 3,
        out_specs=[pl.BlockSpec(memory_space=pltpu.VMEM)] * (heads_here * span),
        out_shape=[shape] * (heads_here * span),
        compiler_params=pltpu.CompilerParams(vmem_limit_bytes=VMEM_LIMIT),
        name="pack_heads",
    )(targets, queries, keys, values)
    return [flat[head * span : (head + 1) * span] for head in range(heads_here)]


def attend(sources, pieces, size):
    rows, columns = pieces[0].shape
    length = rows * len(pieces)
    block = min(256, length)
    blocks = length // block
    scale = size ** (-0.5)

    def kernel(s_ref, *refs):
        *piece_refs, o_ref, x_ref = refs
        for number, piece in enumerate(piece_refs):
            start = pl.multiple_of(s_ref[number] * rows, rows)
            x_ref[pl.ds(start, rows), :] = piece[...]
        row = lax.broadcasted_iota(jnp.int32, (block, block), 0)
        col = lax.broadcasted_iota(jnp.int32, (block, block), 1)
        later = (row > col).astype(jnp.bfloat16)
        causal = col < row
        for qb in range(blocks):
            q_rows = slice(qb * block, (qb + 1) * block)
            query = x_ref[q_rows, 0:size]
            carry = jnp.zeros((block, 1), jnp.float32)
            total = jnp.zeros((block, size), jnp.float32)
            for kb in range(qb, -1, -1):
                k_rows = slice(kb * block, (kb + 1) * block)
                score = scale * lax.dot_general(
                    query,
                    x_ref[k_rows, size : 2 * size],
                    (((1,), (1,)), ((), ())),
                    preferred_element_type=jnp.float32,
                )
                soft = jnp.maximum(score, 0.0) + jnp.log(1.0 + jnp.exp(-jnp.abs(score)))
                rest = score - soft
                if kb == qb:
                    soft = jnp.where(causal, soft, 0.0)
                high = soft.astype(jnp.bfloat16)
                low = (soft - high.astype(jnp.float32)).astype(jnp.bfloat16)
                behind = jnp.dot(high, later, preferred_element_type=jnp.float32)
                behind = behind + jnp.dot(low, later, preferred_element_type=jnp.float32)
                weight = jnp.exp(rest - behind - carry)
                if kb == qb:
                    weight = jnp.where(causal, weight, 0.0)
                total = total + jnp.dot(
                    weight.astype(jnp.bfloat16),
                    x_ref[k_rows, 2 * size : 3 * size],
                    preferred_element_type=jnp.float32,
                )
                if kb > 0:
                    carry = carry + behind[:, 0:1] + soft[:, 0:1]
            o_ref[q_rows, :] = total.astype(o_ref.dtype)

    return pl.pallas_call(
        kernel,
        in_specs=[pl.BlockSpec(memory_space=pltpu.SMEM)]
        + [pl.BlockSpec(memory_space=pltpu.VMEM)] * len(pieces),
        out_specs=pl.BlockSpec(memory_space=pltpu.VMEM),
        out_shape=jax.ShapeDtypeStruct((length, size), pieces[0].dtype),
        scratch_shapes=[pltpu.VMEM((length, columns), pieces[0].dtype)],
        compiler_params=pltpu.CompilerParams(vmem_limit_bytes=VMEM_LIMIT),
        name="attend",
    )(sources, *pieces)


def local_call(kernel, operands, shapes, scratch=(), scalars=0, **more):
    vmem = pl.BlockSpec(memory_space=pltpu.VMEM)
    smem = pl.BlockSpec(memory_space=pltpu.SMEM)
    return pl.pallas_call(
        kernel,
        in_specs=[smem] * scalars + [vmem] * (len(operands) - scalars),
        out_specs=[vmem] * len(shapes),
        out_shape=list(shapes),
        scratch_shapes=list(scratch),
        compiler_params=pltpu.CompilerParams(vmem_limit_bytes=VMEM_LIMIT),
        **more,
    )(*operands)


def finish_rows(place, attended, proj_weight, arrivals, residual, norm_gain, info, part):
    half, width = arrivals[0].shape
    rows = residual.shape[0]
    heads = len(attended)
    size = attended[0].shape[1]

    def kernel(p_ref, *refs):
        att = refs[:heads]
        w_ref, first_ref, second_ref, r_ref, gain_ref, i_ref, stream_ref, normed_ref = refs[heads:]
        mine = slice(part * half, (part + 1) * half)
        start = pl.multiple_of(p_ref[0] * rows + part * half, half)
        total = r_ref[mine, :].astype(jnp.float32)
        total = total + first_ref[...].astype(jnp.float32) + second_ref[...].astype(jnp.float32)
        for head in range(heads):
            total = total + jnp.dot(
                att[head][pl.ds(start, half), :],
                w_ref[head * size : (head + 1) * size, :],
                preferred_element_type=jnp.float32,
            )
        stream = total.astype(jnp.bfloat16)
        stream_ref[...] = stream
        stream = stream.astype(jnp.float32)
        power = jnp.mean(stream * stream, axis=-1, keepdims=True)
        normed = stream * lax.rsqrt(power + EPS) * gain_ref[...]
        normed_ref[:, :width] = normed.astype(jnp.bfloat16)
        normed_ref[:, width:] = i_ref[mine, :]

    return local_call(
        kernel,
        [place, *attended, proj_weight, *arrivals, residual, norm_gain[None], info],
        [
            jax.ShapeDtypeStruct((half, width), jnp.bfloat16),
            jax.ShapeDtypeStruct((half, width + EXTRA), jnp.bfloat16),
        ],
        scalars=1,
        name="finish_rows",
    )


def expert_pair(place, first, second, w_gate, w_up, w_down):
    rows = first.shape[0]
    width = first.shape[1] - EXTRA
    hidden_units = w_gate.shape[1]

    def kernel(p_ref, a_ref, b_ref, g_ref, u_ref, d_ref, oa_ref, ob_ref, x_ref):
        x_ref[:rows] = a_ref[...]
        x_ref[rows:] = b_ref[...]
        x = x_ref[:, :width]
        gate = jnp.dot(x, g_ref[...], preferred_element_type=jnp.float32)
        upper = jnp.dot(x, u_ref[...], preferred_element_type=jnp.float32)
        hidden = (gate / (1.0 + jnp.exp(-gate)) * upper).astype(jnp.bfloat16)
        result = jnp.dot(hidden, d_ref[...], preferred_element_type=jnp.float32)
        info = x_ref[:, width:].astype(jnp.float32)
        expert = p_ref[0].astype(jnp.float32)
        scale = jnp.zeros((2 * rows, 1), jnp.float32)
        for k in range(2):
            name, high, mid, low = (info[:, 4 * k + j : 4 * k + j + 1] for j in range(4))
            scale = scale + jnp.where(name == expert, (low + mid) + high, 0.0)
        out = (result * scale).astype(oa_ref.dtype)
        oa_ref[...] = out[:rows]
        ob_ref[...] = out[rows:]

    shape = jax.ShapeDtypeStruct((rows, width), first.dtype)
    return local_call(
        kernel,
        [place, first, second, w_gate, w_up, w_down],
        [shape, shape],
        [pltpu.VMEM((2 * rows, width + EXTRA), first.dtype)],
        scalars=1,
        cost_estimate=pl.CostEstimate(
            flops=12 * rows * width * hidden_units,
            transcendentals=2 * rows * hidden_units,
            bytes_accessed=6 * width * hidden_units,
        ),
        name="expert_pair",
    )


def combine(streams, owns, arrivals):
    half, width = streams[0].shape

    def kernel(*refs):
        for part in range(2):
            stream, own, arrived = (refs[2 * j + part][...].astype(jnp.float32) for j in range(3))
            refs[6][part * half : (part + 1) * half, :] = (stream + (arrived + own)).astype(jnp.bfloat16)

    shape = jax.ShapeDtypeStruct((2 * half, width), jnp.bfloat16)
    return local_call(kernel, [*streams, *owns, *arrivals], [shape], name="combine")[0]


def body(
    ring,
    queries,
    keys,
    values,
    proj_weight,
    residual,
    norm_gain,
    route,
    route_weight,
    w_gate,
    w_up,
    w_down,
):
    span = lax.axis_size("sp")
    rows, width = queries.shape[1:]
    heads_here = HEADS // span
    size = width // HEADS
    half = rows // 2
    forward = [(ring[i], ring[(i + 1) % span]) for i in range(span)]
    backward = [(b, a) for a, b in forward]
    me = lax.axis_index("sp").astype(jnp.int32)
    place = me[None]
    order = jnp.asarray(np.array(ring, np.int32))
    mine = jnp.asarray(np.argsort(np.array(ring)).astype(np.int32))[me]
    along = order[(mine + np.arange(span, dtype=np.int32)) % span]

    lanes = []
    for k in range(2):
        left = route_weight[0, :, k]
        lanes.append(route[0, :, k].astype(jnp.bfloat16))
        for _ in range(3):
            term = lax.reduce_precision(left, 8, 7)
            lanes.append(term.astype(jnp.bfloat16))
            left = left - term
    info = jnp.pad(jnp.stack(lanes, axis=1), ((0, 0), (0, EXTRA - len(lanes))))

    shifts = sorted(range(span), key=lambda d: (d > 0, abs(d - span // 2)))
    targets = (me + np.array(shifts, np.int32)) % span
    sources = (me - np.array(shifts, np.int32)) % span
    attended = []
    for pieces in pack_heads(targets, queries[0], keys[0], values[0], heads_here, size):
        arrived = [
            lax.ppermute(piece, "sp", [(i, (i + shift) % span) for i in range(span)]) if shift else piece
            for shift, piece in zip(shifts, pieces)
        ]
        attended.append(attend(sources, arrived, size))
    joined = jnp.concatenate(attended, axis=1) if heads_here > 1 else attended[0]

    def projected(offset, part, carried):
        start = along[offset % span] * rows + part * half
        piece = lax.dynamic_slice_in_dim(joined, start, half, 0)
        out = jnp.dot(piece, proj_weight, preferred_element_type=jnp.float32)
        return (out if carried is None else out + carried).astype(jnp.bfloat16)

    reach = span // 2
    travelling = {}
    for distance in range(reach, 0, -1):
        for first in range(2):
            for side, pairs in ((1, forward), (-1, backward)):
                part = first if side == 1 else 1 - first
                if distance == reach and first == 1:
                    continue
                carried = travelling.get((side, part))
                message = projected(side * distance, part, carried)
                travelling[side, part] = lax.ppermute(message, "sp", pairs)

    streams, norms = [], []
    for part in range(2):
        arrivals = [travelling[1, part], travelling[-1, part]]
        stream, normed = finish_rows(
            place, attended, proj_weight, arrivals, residual[0], norm_gain, info, part
        )
        streams.append(stream)
        norms.append(normed)

    def expert(first, second):
        return expert_pair(place, first, second, w_gate[0], w_up[0], w_down[0])

    owns = expert(*norms)
    sums = None
    for step in range(1, span):
        norms = [lax.ppermute(n, "sp", p) for n, p in zip(norms, (forward, backward))]
        outs = expert(*norms)
        if sums is not None:
            outs = [a + b for a, b in zip(sums, outs)]
        sums = [lax.ppermute(o, "sp", p) for o, p in zip(outs, (forward, backward))]
    return combine(streams, owns, sums)[None]


def solution(mesh):
    rows = P("dp", "sp", None)
    return jax.shard_map(
        functools.partial(body, ring_order(mesh)),
        mesh=mesh,
        in_specs=(
            rows,
            rows,
            rows,
            P("sp", None),
            rows,
            P(),
            rows,
            rows,
            P("sp", None, None),
            P("sp", None, None),
            P("sp", None, None),
        ),
        out_specs=rows,
        check_vma=False,
    )
```

```python
import functools
import math

import jax
import jax.numpy as jnp
import numpy as np
from jax import lax
from jax.experimental import pallas as pl
from jax.experimental.pallas import tpu as pltpu
from jax.sharding import PartitionSpec as P

HEADS = 16
EPS = 1e-06
VMEM_LIMIT = 16 << 20
EXTRA = 128


def ring_order(mesh):
    count = mesh.shape["sp"]
    plain = list(range(count))
    try:
        axis = list(mesh.axis_names).index("sp")
        line = np.moveaxis(mesh.devices, axis, 0).reshape(count, -1)[:, 0]
        spots = [tuple(device.coords) for device in line]
    except Exception:
        return plain
    moving = [d for d in range(len(spots[0])) if len({s[d] for s in spots}) > 1]
    if len(moving) != 2:
        return plain
    first, second = sorted(moving, key=lambda d: -len({s[d] for s in spots}))
    where = {(s[first], s[second]): i for i, s in enumerate(spots)}
    rows = sorted({s[first] for s in spots})
    cols = sorted({s[second] for s in spots})
    if len(where) != count or len(rows) * len(cols) != count or len(rows) % 2:
        return plain
    path = []
    for number, row in enumerate(rows):
        inner = cols[1:] if number % 2 == 0 else cols[1:][::-1]
        path.extend((row, col) for col in inner)
    path.extend((row, cols[0]) for row in reversed(rows))
    return [where[spot] for spot in path]


def local_call(kernel, operands, shapes, scratch=(), afar=0, **more):
    vmem = pl.BlockSpec(memory_space=pltpu.VMEM)
    hbm = pl.BlockSpec(memory_space=pltpu.HBM)
    return pl.pallas_call(
        kernel,
        in_specs=[vmem] * (len(operands) - afar) + [hbm] * afar,
        out_specs=[vmem] * len(shapes),
        out_shape=list(shapes),
        scratch_shapes=list(scratch),
        compiler_params=pltpu.CompilerParams(vmem_limit_bytes=VMEM_LIMIT),
        **more,
    )(*operands)


def pack_heads(shifts, queries, keys, values, heads_here, size):
    rows, width = queries.shape
    span = len(shifts)

    def kernel(*refs):
        sources, outs = refs[:3], refs[3 : 3 + heads_here * span]
        held, arrived = refs[-2:]
        me = lax.axis_index("sp")
        copies = [
            pltpu.make_async_copy(source, held.at[part], arrived.at[part])
            for part, source in enumerate(sources)
        ]
        for copy in copies:
            copy.start()
        for part, copy in enumerate(copies):
            copy.wait()
            for number, shift in enumerate(shifts):
                start = lax.rem(me + shift, span) * (heads_here * size)
                for head in range(heads_here):
                    cols = pl.ds(pl.multiple_of(start + head * size, size), size)
                    out = outs[head * span + number]
                    out[:, part * size : (part + 1) * size] = held[part, :, cols]

    shape = jax.ShapeDtypeStruct((rows, 3 * size), queries.dtype)
    flat = pl.pallas_call(
        kernel,
        in_specs=[pl.BlockSpec(memory_space=pltpu.HBM)] * 3,
        out_specs=[pl.BlockSpec(memory_space=pltpu.VMEM)] * (heads_here * span),
        out_shape=[shape] * (heads_here * span),
        scratch_shapes=[
            pltpu.VMEM((3, rows, width), queries.dtype),
            pltpu.SemaphoreType.DMA((3,)),
        ],
        compiler_params=pltpu.CompilerParams(vmem_limit_bytes=VMEM_LIMIT),
        name="pack_heads",
    )(queries, keys, values)
    return [flat[head * span : (head + 1) * span] for head in range(heads_here)]


def attend(shifts, pieces, size, loads=()):
    rows, columns = pieces[0].shape
    span = len(pieces)
    length = rows * span
    block = min(256, length)
    blocks = length // block
    count = len(loads)
    factor = size ** (-0.5) * math.log2(math.e)

    def kernel(*refs):
        piece_refs, refs = refs[:span], refs[span:]
        load_refs, (o_ref, *held_refs) = refs[:count], refs[count : 2 * count + 1]
        x_ref, arrived = refs[-2:]
        copies = [
            pltpu.make_async_copy(source, held, arrived.at[number])
            for number, (source, held) in enumerate(zip(load_refs, held_refs))
        ]
        for copy in copies:
            copy.start()
        me = lax.axis_index("sp")
        for shift, piece in zip(shifts, piece_refs):
            start = pl.multiple_of(lax.rem(me + span - shift, span) * rows, rows)
            x_ref[pl.ds(start, rows), :] = piece[...]
        row = lax.broadcasted_iota(jnp.int32, (block, block), 0)
        col = lax.broadcasted_iota(jnp.int32, (block, block), 1)
        later = (row > col).astype(jnp.bfloat16)
        causal = col < row

        def span_of(number):
            return slice(number * block, (number + 1) * block)

        def scores(qb):
            query = x_ref[span_of(qb), 0:size]
            return [
                lax.dot_general(
                    query,
                    x_ref[span_of(kb), size : 2 * size],
                    (((1,), (1,)), ((), ())),
                    preferred_element_type=jnp.float32,
                )
                for kb in range(qb, -1, -1)
            ]

        def softplus_parts(found):
            parts = []
            for number, score in enumerate(found):
                score = score * factor
                soft = jnp.maximum(score, 0.0) + jnp.log2(1.0 + jnp.exp2(-jnp.abs(score)))
                rest = score - soft
                if number == 0:
                    soft = jnp.where(causal, soft, 0.0)
                parts.append((rest, soft.astype(jnp.bfloat16), soft[:, 0:1]))
            return parts

        def finish(qb, parts, sums):
            carry = total = None
            for number, ((rest, _, first), behind) in enumerate(zip(parts, sums)):
                power = rest - behind
                if carry is not None:
                    power = power - carry
                weight = jnp.exp2(power)
                if number == 0:
                    weight = jnp.where(causal, weight, 0.0)
                part = jnp.dot(
                    weight.astype(jnp.bfloat16),
                    x_ref[span_of(qb - number), 2 * size : 3 * size],
                    preferred_element_type=jnp.float32,
                )
                total = part if total is None else total + part
                passed = behind[:, 0:1] + first
                carry = passed if carry is None else carry + passed
            o_ref[span_of(qb), :] = total.astype(o_ref.dtype)

        found, waiting = scores(0), None
        for qb in range(blocks):
            following = scores(qb + 1) if qb + 1 < blocks else None
            parts = softplus_parts(found)
            sums = [jnp.dot(high, later, preferred_element_type=jnp.float32) for _, high, _ in parts]
            if waiting is not None:
                finish(*waiting)
            waiting, found = (qb, parts, sums), following
        finish(*waiting)
        for copy in copies:
            copy.wait()

    return local_call(
        kernel,
        [*pieces, *loads],
        [
            jax.ShapeDtypeStruct((length, size), pieces[0].dtype),
            *(jax.ShapeDtypeStruct(load.shape, load.dtype) for load in loads),
        ],
        [
            pltpu.VMEM((length, columns), pieces[0].dtype),
            pltpu.SemaphoreType.DMA((max(count, 1),)),
        ],
        afar=count,
        name="attend",
    )


def project_rows(starts, attended, proj_weight, carried, half):
    width = proj_weight.shape[1]
    heads = len(attended)
    size = attended[0].shape[1]

    def kernel(*refs):
        me = lax.axis_index("sp")
        first = starts[0]
        for position, start in enumerate(starts):
            first = lax.select(me == position, start, first)
        first = pl.multiple_of(first, half)
        total = None if carried is None else refs[heads + 1][...].astype(jnp.float32)
        for head in range(heads):
            part = jnp.dot(
                refs[head][pl.ds(first, half), :],
                refs[heads][head * size : (head + 1) * size, :],
                preferred_element_type=jnp.float32,
            )
            total = part if total is None else total + part
        refs[-1][...] = total.astype(jnp.bfloat16)

    return local_call(
        kernel,
        [*attended, proj_weight] + ([] if carried is None else [carried]),
        [jax.ShapeDtypeStruct((half, width), jnp.bfloat16)],
        cost_estimate=pl.CostEstimate(
            flops=2 * half * heads * size * width, transcendentals=0, bytes_accessed=0
        ),
        name="project_rows",
    )[0]


def finish_rows(attended, proj_weight, arrivals, residual, norm_gain, route, route_weight, part):
    half, width = arrivals[0].shape
    rows = residual.shape[0]
    heads = len(attended)
    size = attended[0].shape[1]

    def kernel(*refs):
        att = refs[:heads]
        w_ref, first_ref, second_ref, r_ref, gain_ref, n_ref, s_ref = refs[heads:-2]
        stream_ref, normed_ref = refs[-2:]
        mine = slice(part * half, (part + 1) * half)
        start = pl.multiple_of(lax.axis_index("sp") * rows + part * half, half)
        total = r_ref[mine, :].astype(jnp.float32)
        total = total + first_ref[...].astype(jnp.float32) + second_ref[...].astype(jnp.float32)
        for head in range(heads):
            total = total + jnp.dot(
                att[head][pl.ds(start, half), :],
                w_ref[head * size : (head + 1) * size, :],
                preferred_element_type=jnp.float32,
            )
        stream = total.astype(jnp.bfloat16)
        stream_ref[...] = stream
        stream = stream.astype(jnp.float32)
        power = jnp.mean(stream * stream, axis=-1, keepdims=True)
        normed = stream * lax.rsqrt(power + EPS) * gain_ref[...]
        normed_ref[:, :width] = normed.astype(jnp.bfloat16)
        lines = []
        for k in range(2):
            lines.append(n_ref[k : k + 1, :].astype(jnp.float32))
            left = s_ref[k : k + 1, :]
            for _ in range(3):
                lines.append(left.astype(jnp.bfloat16).astype(jnp.float32))
                left = left - lines[-1]
        table = jnp.zeros((EXTRA, rows), jnp.float32)
        which = lax.broadcasted_iota(jnp.int32, (EXTRA, rows), 0)
        for number, line in enumerate(lines):
            table = jnp.where(which == number, line, table)
        normed_ref[:, width:] = table.T[mine, :].astype(jnp.bfloat16)

    return local_call(
        kernel,
        [*attended, proj_weight, *arrivals, residual, norm_gain[None], route.T, route_weight.T],
        [
            jax.ShapeDtypeStruct((half, width), jnp.bfloat16),
            jax.ShapeDtypeStruct((half, width + EXTRA), jnp.bfloat16),
        ],
        name="finish_rows",
    )


def expert_pair(first, second, w_gate, w_up, w_down):
    rows = first.shape[0]
    width = first.shape[1] - EXTRA
    hidden_units = w_gate.shape[1]

    def kernel(a_ref, b_ref, g_ref, u_ref, d_ref, oa_ref, ob_ref, x_ref):
        x_ref[:rows] = a_ref[...]
        x_ref[rows:] = b_ref[...]
        x = x_ref[:, :width]
        gate = jnp.dot(x, g_ref[...], preferred_element_type=jnp.float32)
        upper = jnp.dot(x, u_ref[...], preferred_element_type=jnp.float32)
        hidden = (gate / (1.0 + jnp.exp(-gate)) * upper).astype(jnp.bfloat16)
        result = jnp.dot(hidden, d_ref[...], preferred_element_type=jnp.float32)
        info = x_ref[:, width:].astype(jnp.float32)
        expert = lax.axis_index("sp").astype(jnp.float32)
        scale = jnp.zeros((2 * rows, 1), jnp.float32)
        for k in range(2):
            name, high, mid, low = (info[:, 4 * k + j : 4 * k + j + 1] for j in range(4))
            scale = scale + jnp.where(name == expert, (low + mid) + high, 0.0)
        out = (result * scale).astype(oa_ref.dtype)
        oa_ref[...] = out[:rows]
        ob_ref[...] = out[rows:]

    shape = jax.ShapeDtypeStruct((rows, width), first.dtype)
    return local_call(
        kernel,
        [first, second, w_gate, w_up, w_down],
        [shape, shape],
        [pltpu.VMEM((2 * rows, width + EXTRA), first.dtype)],
        cost_estimate=pl.CostEstimate(
            flops=12 * rows * width * hidden_units,
            transcendentals=2 * rows * hidden_units,
            bytes_accessed=6 * width * hidden_units,
        ),
        name="expert_pair",
    )


def combine(streams, owns, arrivals):
    half, width = streams[0].shape

    def kernel(*refs):
        for part in range(2):
            stream, own, arrived = (refs[2 * j + part][...].astype(jnp.float32) for j in range(3))
            refs[6][part * half : (part + 1) * half, :] = (stream + (arrived + own)).astype(jnp.bfloat16)

    shape = jax.ShapeDtypeStruct((2 * half, width), jnp.bfloat16)
    return local_call(kernel, [*streams, *owns, *arrivals], [shape], name="combine")[0]


def body(
    ring,
    queries,
    keys,
    values,
    proj_weight,
    residual,
    norm_gain,
    route,
    route_weight,
    w_gate,
    w_up,
    w_down,
):
    span = lax.axis_size("sp")
    rows, width = queries.shape[1:]
    heads_here = HEADS // span
    size = width // HEADS
    half = rows // 2
    forward = [(ring[i], ring[(i + 1) % span]) for i in range(span)]
    backward = [(b, a) for a, b in forward]
    mine = [ring.index(position) for position in range(span)]

    shifts = sorted(range(span), key=lambda d: (d > 0, abs(d - span // 2)))
    attended = []
    weights = (w_gate[0], w_up[0], w_down[0])
    for pieces in pack_heads(shifts, queries[0], keys[0], values[0], heads_here, size):
        arrived = [
            lax.ppermute(piece, "sp", [(i, (i + shift) % span) for i in range(span)]) if shift else piece
            for shift, piece in zip(shifts, pieces)
        ]
        result, *loaded = attend(shifts, arrived, size, ())
        attended.append(result)
        weights = loaded or weights

    def projected(offset, part, carried):
        starts = [ring[(spot + offset) % span] * rows + part * half for spot in mine]
        return project_rows(starts, attended, proj_weight, carried, half)

    reach = span // 2
    travelling, message = {}, {}
    for distance in range(reach, 0, -1):
        for first in (1, 0) if distance < reach else (0,):
            for side, pairs in ((1, forward), (-1, backward)):
                part = first if side == 1 else 1 - first
                carried = travelling.get((side, part))
                sent = projected(side * distance, part, carried)
                if first == 1:
                    message[side] = sent
                travelling[side, part] = lax.ppermute(sent, "sp", pairs)

    streams, norms = [], []
    for part in range(2):
        arrivals = [travelling[1, part], travelling[-1, part]]
        stream, normed = finish_rows(
            attended, proj_weight, arrivals, residual[0], norm_gain, route[0], route_weight[0], part
        )
        streams.append(stream)
        norms.append(normed)

    def expert(first, second):
        return expert_pair(first, second, *weights)

    owns = expert(*norms)
    sums = None
    for step in range(1, span):
        norms = [lax.ppermute(n, "sp", p) for n, p in zip(norms, (forward, backward))]
        outs = expert(*norms)
        if sums is not None:
            outs = [a + b for a, b in zip(sums, outs)]
        sums = [lax.ppermute(o, "sp", p) for o, p in zip(outs, (forward, backward))]
    return combine(streams, owns, sums)[None]


def solution(mesh):
    rows = P("dp", "sp", None)
    return jax.shard_map(
        functools.partial(body, ring_order(mesh)),
        mesh=mesh,
        in_specs=(
            rows,
            rows,
            rows,
            P("sp", None),
            rows,
            P(),
            rows,
            rows,
            P("sp", None, None),
            P("sp", None, None),
            P("sp", None, None),
        ),
        out_specs=rows,
        check_vma=False,
    )
```

```python
import functools
import math

import jax
import jax.numpy as jnp
import numpy as np
from jax import lax
from jax.experimental import pallas as pl
from jax.experimental.pallas import tpu as pltpu
from jax.sharding import PartitionSpec as P

HEADS = 16
EPS = 1e-06
VMEM_LIMIT = 16 << 20
EXTRA = 128


def ring_order(mesh):
    count = mesh.shape["sp"]
    plain = list(range(count))
    try:
        axis = list(mesh.axis_names).index("sp")
        line = np.moveaxis(mesh.devices, axis, 0).reshape(count, -1)[:, 0]
        spots = [tuple(device.coords) for device in line]
    except Exception:
        return plain
    moving = [d for d in range(len(spots[0])) if len({s[d] for s in spots}) > 1]
    if len(moving) != 2:
        return plain
    first, second = sorted(moving, key=lambda d: -len({s[d] for s in spots}))
    where = {(s[first], s[second]): i for i, s in enumerate(spots)}
    rows = sorted({s[first] for s in spots})
    cols = sorted({s[second] for s in spots})
    if len(where) != count or len(rows) * len(cols) != count or len(rows) % 2:
        return plain
    path = []
    for number, row in enumerate(rows):
        inner = cols[1:] if number % 2 == 0 else cols[1:][::-1]
        path.extend((row, col) for col in inner)
    path.extend((row, cols[0]) for row in reversed(rows))
    return [where[spot] for spot in path]


def local_call(kernel, operands, shapes, scratch=(), afar=0, **more):
    vmem = pl.BlockSpec(memory_space=pltpu.VMEM)
    hbm = pl.BlockSpec(memory_space=pltpu.HBM)
    return pl.pallas_call(
        kernel,
        in_specs=[vmem] * (len(operands) - afar) + [hbm] * afar,
        out_specs=[vmem] * len(shapes),
        out_shape=list(shapes),
        scratch_shapes=list(scratch),
        compiler_params=pltpu.CompilerParams(vmem_limit_bytes=VMEM_LIMIT),
        **more,
    )(*operands)


def pack_heads(shifts, queries, keys, values, heads_here, size):
    rows, width = queries.shape
    span = len(shifts)

    def kernel(*refs):
        sources, outs = refs[:3], refs[3 : 3 + heads_here * span]
        held, arrived = refs[-2:]
        me = lax.axis_index("sp")
        copies = [
            pltpu.make_async_copy(source, held.at[part], arrived.at[part])
            for part, source in enumerate(sources)
        ]
        for copy in copies:
            copy.start()
        for part, copy in enumerate(copies):
            copy.wait()
            for number, shift in enumerate(shifts):
                start = lax.rem(me + shift, span) * (heads_here * size)
                for head in range(heads_here):
                    cols = pl.ds(pl.multiple_of(start + head * size, size), size)
                    out = outs[head * span + number]
                    out[:, part * size : (part + 1) * size] = held[part, :, cols]

    shape = jax.ShapeDtypeStruct((rows, 3 * size), queries.dtype)
    flat = pl.pallas_call(
        kernel,
        in_specs=[pl.BlockSpec(memory_space=pltpu.HBM)] * 3,
        out_specs=[pl.BlockSpec(memory_space=pltpu.VMEM)] * (heads_here * span),
        out_shape=[shape] * (heads_here * span),
        scratch_shapes=[
            pltpu.VMEM((3, rows, width), queries.dtype),
            pltpu.SemaphoreType.DMA((3,)),
        ],
        compiler_params=pltpu.CompilerParams(vmem_limit_bytes=VMEM_LIMIT),
        name="pack_heads",
    )(*(pltpu.with_memory_space_constraint(x, pltpu.HBM) for x in (queries, keys, values)))
    return [flat[head * span : (head + 1) * span] for head in range(heads_here)]


def attend(shifts, pieces, size, loads=()):
    rows, columns = pieces[0].shape
    span = len(pieces)
    length = rows * span
    block = min(256, length)
    blocks = length // block
    count = len(loads)
    factor = size ** (-0.5) * math.log2(math.e)

    def kernel(*refs):
        piece_refs, refs = refs[:span], refs[span:]
        load_refs, (o_ref, *held_refs) = refs[:count], refs[count : 2 * count + 1]
        x_ref, arrived = refs[-2:]
        copies = [
            pltpu.make_async_copy(source, held, arrived.at[number])
            for number, (source, held) in enumerate(zip(load_refs, held_refs))
        ]
        for copy in copies:
            copy.start()
        me = lax.axis_index("sp")
        for shift, piece in zip(shifts, piece_refs):
            start = pl.multiple_of(lax.rem(me + span - shift, span) * rows, rows)
            x_ref[pl.ds(start, rows), :] = piece[...]
        row = lax.broadcasted_iota(jnp.int32, (block, block), 0)
        col = lax.broadcasted_iota(jnp.int32, (block, block), 1)
        later = (row > col).astype(jnp.bfloat16)
        causal = col < row

        def span_of(number):
            return slice(number * block, (number + 1) * block)

        def scores(qb):
            query = x_ref[span_of(qb), 0:size]
            return [
                lax.dot_general(
                    query,
                    x_ref[span_of(kb), size : 2 * size],
                    (((1,), (1,)), ((), ())),
                    preferred_element_type=jnp.float32,
                )
                for kb in range(qb, -1, -1)
            ]

        def softplus_parts(found):
            parts = []
            for number, score in enumerate(found):
                score = score * factor
                soft = jnp.maximum(score, 0.0) + jnp.log2(1.0 + jnp.exp2(-jnp.abs(score)))
                rest = score - soft
                if number == 0:
                    soft = jnp.where(causal, soft, 0.0)
                parts.append((rest, soft.astype(jnp.bfloat16), soft[:, 0:1]))
            return parts

        def finish(qb, parts, sums):
            carry = total = None
            for number, ((rest, _, first), behind) in enumerate(zip(parts, sums)):
                power = rest - behind
                if carry is not None:
                    power = power - carry
                weight = jnp.exp2(power)
                if number == 0:
                    weight = jnp.where(causal, weight, 0.0)
                part = jnp.dot(
                    weight.astype(jnp.bfloat16),
                    x_ref[span_of(qb - number), 2 * size : 3 * size],
                    preferred_element_type=jnp.float32,
                )
                total = part if total is None else total + part
                passed = behind[:, 0:1] + first
                carry = passed if carry is None else carry + passed
            o_ref[span_of(qb), :] = total.astype(o_ref.dtype)

        found, waiting = scores(0), None
        for qb in range(blocks):
            following = scores(qb + 1) if qb + 1 < blocks else None
            parts = softplus_parts(found)
            sums = [jnp.dot(high, later, preferred_element_type=jnp.float32) for _, high, _ in parts]
            if waiting is not None:
                finish(*waiting)
            waiting, found = (qb, parts, sums), following
        finish(*waiting)
        for copy in copies:
            copy.wait()

    return local_call(
        kernel,
        [*pieces, *loads],
        [
            jax.ShapeDtypeStruct((length, size), pieces[0].dtype),
            *(jax.ShapeDtypeStruct(load.shape, load.dtype) for load in loads),
        ],
        [
            pltpu.VMEM((length, columns), pieces[0].dtype),
            pltpu.SemaphoreType.DMA((max(count, 1),)),
        ],
        afar=count,
        name="attend",
    )


def project_rows(starts, attended, proj_weight, carried, half):
    width = proj_weight.shape[1]
    heads = len(attended)
    size = attended[0].shape[1]

    def kernel(*refs):
        me = lax.axis_index("sp")
        first = starts[0]
        for position, start in enumerate(starts):
            first = lax.select(me == position, start, first)
        first = pl.multiple_of(first, half)
        total = None if carried is None else refs[heads + 1][...].astype(jnp.float32)
        for head in range(heads):
            part = jnp.dot(
                refs[head][pl.ds(first, half), :],
                refs[heads][head * size : (head + 1) * size, :],
                preferred_element_type=jnp.float32,
            )
            total = part if total is None else total + part
        refs[-1][...] = total.astype(jnp.bfloat16)

    return local_call(
        kernel,
        [*attended, proj_weight] + ([] if carried is None else [carried]),
        [jax.ShapeDtypeStruct((half, width), jnp.bfloat16)],
        cost_estimate=pl.CostEstimate(
            flops=2 * half * heads * size * width, transcendentals=0, bytes_accessed=0
        ),
        name="project_rows",
    )[0]


def finish_rows(attended, proj_weight, arrivals, residual, norm_gain, route, route_weight, part):
    half, width = arrivals[0].shape
    rows = residual.shape[0]
    heads = len(attended)
    size = attended[0].shape[1]

    def kernel(*refs):
        att = refs[:heads]
        w_ref, first_ref, second_ref, r_ref, gain_ref, n_ref, s_ref = refs[heads:-2]
        stream_ref, normed_ref = refs[-2:]
        mine = slice(part * half, (part + 1) * half)
        start = pl.multiple_of(lax.axis_index("sp") * rows + part * half, half)
        total = r_ref[mine, :].astype(jnp.float32)
        total = total + first_ref[...].astype(jnp.float32) + second_ref[...].astype(jnp.float32)
        for head in range(heads):
            total = total + jnp.dot(
                att[head][pl.ds(start, half), :],
                w_ref[head * size : (head + 1) * size, :],
                preferred_element_type=jnp.float32,
            )
        stream = total.astype(jnp.bfloat16)
        stream_ref[...] = stream
        stream = stream.astype(jnp.float32)
        power = jnp.mean(stream * stream, axis=-1, keepdims=True)
        normed = stream * lax.rsqrt(power + EPS) * gain_ref[...]
        normed_ref[:, :width] = normed.astype(jnp.bfloat16)
        lines = []
        for k in range(2):
            lines.append(n_ref[k : k + 1, :].astype(jnp.float32))
            left = s_ref[k : k + 1, :]
            for _ in range(3):
                lines.append(left.astype(jnp.bfloat16).astype(jnp.float32))
                left = left - lines[-1]
        table = jnp.zeros((EXTRA, rows), jnp.float32)
        which = lax.broadcasted_iota(jnp.int32, (EXTRA, rows), 0)
        for number, line in enumerate(lines):
            table = jnp.where(which == number, line, table)
        normed_ref[:, width:] = table.T[mine, :].astype(jnp.bfloat16)

    return local_call(
        kernel,
        [*attended, proj_weight, *arrivals, residual, norm_gain[None], route.T, route_weight.T],
        [
            jax.ShapeDtypeStruct((half, width), jnp.bfloat16),
            jax.ShapeDtypeStruct((half, width + EXTRA), jnp.bfloat16),
        ],
        name="finish_rows",
    )


def expert_pair(first, second, w_gate, w_up, w_down):
    rows = first.shape[0]
    width = first.shape[1] - EXTRA
    hidden_units = w_gate.shape[1]

    def kernel(a_ref, b_ref, g_ref, u_ref, d_ref, oa_ref, ob_ref, x_ref):
        x_ref[:rows] = a_ref[...]
        x_ref[rows:] = b_ref[...]
        x = x_ref[:, :width]
        gate = jnp.dot(x, g_ref[...], preferred_element_type=jnp.float32)
        upper = jnp.dot(x, u_ref[...], preferred_element_type=jnp.float32)
        hidden = (gate / (1.0 + jnp.exp(-gate)) * upper).astype(jnp.bfloat16)
        result = jnp.dot(hidden, d_ref[...], preferred_element_type=jnp.float32)
        info = x_ref[:, width:].astype(jnp.float32)
        expert = lax.axis_index("sp").astype(jnp.float32)
        scale = jnp.zeros((2 * rows, 1), jnp.float32)
        for k in range(2):
            name, high, mid, low = (info[:, 4 * k + j : 4 * k + j + 1] for j in range(4))
            scale = scale + jnp.where(name == expert, (low + mid) + high, 0.0)
        out = (result * scale).astype(oa_ref.dtype)
        oa_ref[...] = out[:rows]
        ob_ref[...] = out[rows:]

    shape = jax.ShapeDtypeStruct((rows, width), first.dtype)
    return local_call(
        kernel,
        [first, second, w_gate, w_up, w_down],
        [shape, shape],
        [pltpu.VMEM((2 * rows, width + EXTRA), first.dtype)],
        cost_estimate=pl.CostEstimate(
            flops=12 * rows * width * hidden_units,
            transcendentals=2 * rows * hidden_units,
            bytes_accessed=6 * width * hidden_units,
        ),
        name="expert_pair",
    )


def combine(streams, owns, arrivals):
    half, width = streams[0].shape

    def kernel(*refs):
        for part in range(2):
            stream, own, arrived = (refs[2 * j + part][...].astype(jnp.float32) for j in range(3))
            refs[6][part * half : (part + 1) * half, :] = (stream + (arrived + own)).astype(jnp.bfloat16)

    shape = jax.ShapeDtypeStruct((2 * half, width), jnp.bfloat16)
    return local_call(kernel, [*streams, *owns, *arrivals], [shape], name="combine")[0]


def body(
    ring,
    queries,
    keys,
    values,
    proj_weight,
    residual,
    norm_gain,
    route,
    route_weight,
    w_gate,
    w_up,
    w_down,
):
    span = lax.axis_size("sp")
    rows, width = queries.shape[1:]
    heads_here = HEADS // span
    size = width // HEADS
    half = rows // 2
    forward = [(ring[i], ring[(i + 1) % span]) for i in range(span)]
    backward = [(b, a) for a, b in forward]
    mine = [ring.index(position) for position in range(span)]

    shifts = sorted(range(span), key=lambda d: (d > 0, abs(d - span // 2)))
    attended = []
    weights = (w_gate[0], w_up[0], w_down[0])
    for pieces in pack_heads(shifts, queries[0], keys[0], values[0], heads_here, size):
        arrived = [
            lax.ppermute(piece, "sp", [(i, (i + shift) % span) for i in range(span)]) if shift else piece
            for shift, piece in zip(shifts, pieces)
        ]
        result, *loaded = attend(shifts, arrived, size, ())
        attended.append(result)
        weights = loaded or weights

    def projected(offset, part, carried):
        starts = [ring[(spot + offset) % span] * rows + part * half for spot in mine]
        return project_rows(starts, attended, proj_weight, carried, half)

    reach = span // 2
    travelling, message = {}, {}
    for distance in range(reach, 0, -1):
        for first in (1, 0) if distance < reach else (0,):
            for side, pairs in ((1, forward), (-1, backward)):
                part = first if side == 1 else 1 - first
                carried = travelling.get((side, part))
                sent = projected(side * distance, part, carried)
                if first == 1:
                    message[side] = sent
                travelling[side, part] = lax.ppermute(sent, "sp", pairs)

    streams, norms = [], []
    for part in range(2):
        arrivals = [travelling[1, part], travelling[-1, part]]
        stream, normed = finish_rows(
            attended, proj_weight, arrivals, residual[0], norm_gain, route[0], route_weight[0], part
        )
        streams.append(stream)
        norms.append(normed)

    def expert(first, second):
        return expert_pair(first, second, *weights)

    owns = expert(*norms)
    sums = None
    for step in range(1, span):
        norms = [lax.ppermute(n, "sp", p) for n, p in zip(norms, (forward, backward))]
        outs = expert(*norms)
        if sums is not None:
            outs = [a + b for a, b in zip(sums, outs)]
        sums = [lax.ppermute(o, "sp", p) for o, p in zip(outs, (forward, backward))]
    return combine(streams, owns, sums)[None]


def solution(mesh):
    rows = P("dp", "sp", None)
    return jax.shard_map(
        functools.partial(body, ring_order(mesh)),
        mesh=mesh,
        in_specs=(
            rows,
            rows,
            rows,
            P("sp", None),
            rows,
            P(),
            rows,
            rows,
            P("sp", None, None),
            P("sp", None, None),
            P("sp", None, None),
        ),
        out_specs=rows,
        check_vma=False,
    )
```

```python
import functools
import math

import jax
import jax.numpy as jnp
import numpy as np
from jax import lax
from jax.experimental import pallas as pl
from jax.experimental.pallas import tpu as pltpu
from jax.sharding import PartitionSpec as P

HEADS = 16
EPS = 1e-06
VMEM_LIMIT = 16 << 20
EXTRA = 16


def ring_order(mesh):
    count = mesh.shape["sp"]
    plain = list(range(count))
    try:
        axis = list(mesh.axis_names).index("sp")
        line = np.moveaxis(mesh.devices, axis, 0).reshape(count, -1)[:, 0]
        spots = [tuple(device.coords) for device in line]
    except Exception:
        return plain
    moving = [d for d in range(len(spots[0])) if len({s[d] for s in spots}) > 1]
    if len(moving) != 2:
        return plain
    first, second = sorted(moving, key=lambda d: -len({s[d] for s in spots}))
    where = {(s[first], s[second]): i for i, s in enumerate(spots)}
    rows = sorted({s[first] for s in spots})
    cols = sorted({s[second] for s in spots})
    if len(where) != count or len(rows) * len(cols) != count or len(rows) % 2:
        return plain
    path = []
    for number, row in enumerate(rows):
        inner = cols[1:] if number % 2 == 0 else cols[1:][::-1]
        path.extend((row, col) for col in inner)
    path.extend((row, cols[0]) for row in reversed(rows))
    return [where[spot] for spot in path]


def local_call(kernel, operands, shapes, scratch=(), afar=0, **more):
    vmem = pl.BlockSpec(memory_space=pltpu.VMEM)
    hbm = pl.BlockSpec(memory_space=pltpu.HBM)
    return pl.pallas_call(
        kernel,
        in_specs=[vmem] * (len(operands) - afar) + [hbm] * afar,
        out_specs=[vmem] * len(shapes),
        out_shape=list(shapes),
        scratch_shapes=list(scratch),
        compiler_params=pltpu.CompilerParams(vmem_limit_bytes=VMEM_LIMIT),
        **more,
    )(*operands)


def pack_heads(shifts, queries, keys, values, heads_here, size):
    rows, width = queries.shape
    span = len(shifts)

    def kernel(*refs):
        sources, outs = refs[:3], refs[3 : 3 + heads_here * span]
        held, arrived = refs[-2:]
        me = lax.axis_index("sp")
        copies = [
            pltpu.make_async_copy(source, held.at[part], arrived.at[part])
            for part, source in enumerate(sources)
        ]
        for copy in copies:
            copy.start()
        for part, copy in enumerate(copies):
            copy.wait()
            for number, shift in enumerate(shifts):
                start = lax.rem(me + shift, span) * (heads_here * size)
                for head in range(heads_here):
                    cols = pl.ds(pl.multiple_of(start + head * size, size), size)
                    out = outs[head * span + number]
                    out[:, part * size : (part + 1) * size] = held[part, :, cols]

    shape = jax.ShapeDtypeStruct((rows, 3 * size), queries.dtype)
    flat = pl.pallas_call(
        kernel,
        in_specs=[pl.BlockSpec(memory_space=pltpu.HBM)] * 3,
        out_specs=[pl.BlockSpec(memory_space=pltpu.VMEM)] * (heads_here * span),
        out_shape=[shape] * (heads_here * span),
        scratch_shapes=[
            pltpu.VMEM((3, rows, width), queries.dtype),
            pltpu.SemaphoreType.DMA((3,)),
        ],
        compiler_params=pltpu.CompilerParams(vmem_limit_bytes=VMEM_LIMIT),
        name="pack_heads",
    )(*(pltpu.with_memory_space_constraint(x, pltpu.HBM) for x in (queries, keys, values)))
    return [flat[head * span : (head + 1) * span] for head in range(heads_here)]


def attend(shifts, pieces, size, loads=()):
    rows, columns = pieces[0].shape
    span = len(pieces)
    length = rows * span
    block = min(256, length)
    blocks = length // block
    count = len(loads)
    factor = size ** (-0.5) * math.log2(math.e)

    def kernel(*refs):
        piece_refs, refs = refs[:span], refs[span:]
        load_refs, (o_ref, *held_refs) = refs[:count], refs[count : 2 * count + 1]
        x_ref, arrived = refs[-2:]
        copies = [
            pltpu.make_async_copy(source, held, arrived.at[number])
            for number, (source, held) in enumerate(zip(load_refs, held_refs))
        ]
        for copy in copies:
            copy.start()
        me = lax.axis_index("sp")
        for shift, piece in zip(shifts, piece_refs):
            start = pl.multiple_of(lax.rem(me + span - shift, span) * rows, rows)
            x_ref[pl.ds(start, rows), :] = piece[...]
        row = lax.broadcasted_iota(jnp.int32, (block, block), 0)
        col = lax.broadcasted_iota(jnp.int32, (block, block), 1)
        later = (row > col).astype(jnp.bfloat16)
        causal = col < row

        def span_of(number):
            return slice(number * block, (number + 1) * block)

        def scores(qb):
            query = x_ref[span_of(qb), 0:size]
            return [
                lax.dot_general(
                    query,
                    x_ref[span_of(kb), size : 2 * size],
                    (((1,), (1,)), ((), ())),
                    preferred_element_type=jnp.float32,
                )
                for kb in range(qb, -1, -1)
            ]

        def softplus_parts(found):
            parts = []
            for number, score in enumerate(found):
                score = score * factor
                soft = jnp.maximum(score, 0.0) + jnp.log2(1.0 + jnp.exp2(-jnp.abs(score)))
                rest = score - soft
                if number == 0:
                    soft = jnp.where(causal, soft, 0.0)
                parts.append((rest, soft.astype(jnp.bfloat16), soft[:, 0:1]))
            return parts

        def finish(qb, parts, sums):
            carry = total = None
            for number, ((rest, _, first), behind) in enumerate(zip(parts, sums)):
                power = rest - behind
                if carry is not None:
                    power = power - carry
                weight = jnp.exp2(power)
                if number == 0:
                    weight = jnp.where(causal, weight, 0.0)
                part = jnp.dot(
                    weight.astype(jnp.bfloat16),
                    x_ref[span_of(qb - number), 2 * size : 3 * size],
                    preferred_element_type=jnp.float32,
                )
                total = part if total is None else total + part
                passed = behind[:, 0:1] + first
                carry = passed if carry is None else carry + passed
            o_ref[span_of(qb), :] = total.astype(o_ref.dtype)

        found, waiting = scores(0), None
        for qb in range(blocks):
            following = scores(qb + 1) if qb + 1 < blocks else None
            parts = softplus_parts(found)
            sums = [jnp.dot(high, later, preferred_element_type=jnp.float32) for _, high, _ in parts]
            if waiting is not None:
                finish(*waiting)
            waiting, found = (qb, parts, sums), following
        finish(*waiting)
        for copy in copies:
            copy.wait()

    return local_call(
        kernel,
        [*pieces, *loads],
        [
            jax.ShapeDtypeStruct((length, size), pieces[0].dtype),
            *(jax.ShapeDtypeStruct(load.shape, load.dtype) for load in loads),
        ],
        [
            pltpu.VMEM((length, columns), pieces[0].dtype),
            pltpu.SemaphoreType.DMA((max(count, 1),)),
        ],
        afar=count,
        name="attend",
    )


def project_rows(starts, attended, proj_weight, carried, half):
    width = proj_weight.shape[1]
    heads = len(attended)
    size = attended[0].shape[1]

    def kernel(*refs):
        me = lax.axis_index("sp")
        first = starts[0]
        for position, start in enumerate(starts):
            first = lax.select(me == position, start, first)
        first = pl.multiple_of(first, half)
        total = None if carried is None else refs[heads + 1][...].astype(jnp.float32)
        for head in range(heads):
            part = jnp.dot(
                refs[head][pl.ds(first, half), :],
                refs[heads][head * size : (head + 1) * size, :],
                preferred_element_type=jnp.float32,
            )
            total = part if total is None else total + part
        refs[-1][...] = total.astype(jnp.bfloat16)

    return local_call(
        kernel,
        [*attended, proj_weight] + ([] if carried is None else [carried]),
        [jax.ShapeDtypeStruct((half, width), jnp.bfloat16)],
        cost_estimate=pl.CostEstimate(
            flops=2 * half * heads * size * width, transcendentals=0, bytes_accessed=0
        ),
        name="project_rows",
    )[0]


def finish_rows(attended, proj_weight, arrivals, residual, norm_gain, route, route_weight, part):
    half, width = arrivals[0].shape
    rows = residual.shape[0]
    heads = len(attended)
    size = attended[0].shape[1]

    def kernel(*refs):
        att = refs[:heads]
        w_ref, first_ref, second_ref, r_ref, gain_ref, n_ref, s_ref = refs[heads:-2]
        stream_ref, normed_ref = refs[-2:]
        mine = slice(part * half, (part + 1) * half)
        start = pl.multiple_of(lax.axis_index("sp") * rows + part * half, half)
        total = r_ref[mine, :].astype(jnp.float32)
        total = total + first_ref[...].astype(jnp.float32) + second_ref[...].astype(jnp.float32)
        for head in range(heads):
            total = total + jnp.dot(
                att[head][pl.ds(start, half), :],
                w_ref[head * size : (head + 1) * size, :],
                preferred_element_type=jnp.float32,
            )
        stream = total.astype(jnp.bfloat16)
        stream_ref[...] = stream
        stream = stream.astype(jnp.float32)
        power = jnp.mean(stream * stream, axis=-1, keepdims=True)
        normed = stream * lax.rsqrt(power + EPS) * gain_ref[...]
        normed = normed.astype(jnp.bfloat16)
        for number in range(width // rows):
            to = slice(number * half, (number + 1) * half)
            normed_ref[to, :] = normed[:, number * rows : (number + 1) * rows]
        lines = []
        for k in range(2):
            lines.append(n_ref[k : k + 1, :].astype(jnp.float32))
            left = s_ref[k : k + 1, :]
            for _ in range(3):
                lines.append(left.astype(jnp.bfloat16).astype(jnp.float32))
                left = left - lines[-1]
        table = jnp.zeros((EXTRA, rows), jnp.float32)
        which = lax.broadcasted_iota(jnp.int32, (EXTRA, rows), 0)
        for number, line in enumerate(lines):
            table = jnp.where(which == number, line, table)
        lane = lax.broadcasted_iota(jnp.int32, (EXTRA, rows), 1)
        table = jnp.where((lane >= half) == bool(part), table, 0.0)
        normed_ref[width // rows * half :, :] = table.astype(jnp.bfloat16)

    return local_call(
        kernel,
        [*attended, proj_weight, *arrivals, residual, norm_gain[None], route.T, route_weight.T],
        [
            jax.ShapeDtypeStruct((half, width), jnp.bfloat16),
            jax.ShapeDtypeStruct((width // rows * half + EXTRA, rows), jnp.bfloat16),
        ],
        name="finish_rows",
    )


def expert_pair(first, second, w_gate, w_up, w_down):
    lanes = first.shape[1]
    rows = lanes // 2
    width, hidden_units = w_gate.shape

    def kernel(a_ref, b_ref, g_ref, u_ref, d_ref, oa_ref, ob_ref, x_ref):
        for part, ref in enumerate((a_ref, b_ref)):
            for number in range(width // lanes):
                cols = slice(number * lanes, (number + 1) * lanes)
                x_ref[part * rows : (part + 1) * rows, cols] = ref[number * rows : (number + 1) * rows, :]
        x = x_ref[...]
        gate = jnp.dot(x, g_ref[...], preferred_element_type=jnp.float32)
        upper = jnp.dot(x, u_ref[...], preferred_element_type=jnp.float32)
        hidden = (gate / (1.0 + jnp.exp(-gate)) * upper).astype(jnp.bfloat16)
        result = jnp.dot(hidden, d_ref[...], preferred_element_type=jnp.float32)
        below = slice(width // lanes * rows, width // lanes * rows + EXTRA)
        info = a_ref[below, :].astype(jnp.float32) + b_ref[below, :].astype(jnp.float32)
        expert = lax.axis_index("sp").astype(jnp.float32)
        line = jnp.zeros((1, lanes), jnp.float32)
        for k in range(2):
            name, high, mid, low = (info[4 * k + j : 4 * k + j + 1, :] for j in range(4))
            line = line + jnp.where(name == expert, (low + mid) + high, 0.0)
        scale = jnp.broadcast_to(line, (lanes, lanes)).T[:, 0:1]
        out = (result * scale).astype(oa_ref.dtype)
        oa_ref[...] = out[:rows]
        ob_ref[...] = out[rows:]

    shape = jax.ShapeDtypeStruct((rows, width), first.dtype)
    return local_call(
        kernel,
        [first, second, w_gate, w_up, w_down],
        [shape, shape],
        [pltpu.VMEM((2 * rows, width), first.dtype)],
        cost_estimate=pl.CostEstimate(
            flops=12 * rows * width * hidden_units,
            transcendentals=2 * rows * hidden_units,
            bytes_accessed=6 * width * hidden_units,
        ),
        name="expert_pair",
    )


def combine(streams, owns, arrivals):
    half, width = streams[0].shape

    def kernel(*refs):
        for part in range(2):
            stream, own, arrived = (refs[2 * j + part][...].astype(jnp.float32) for j in range(3))
            refs[6][part * half : (part + 1) * half, :] = (stream + (arrived + own)).astype(jnp.bfloat16)

    shape = jax.ShapeDtypeStruct((2 * half, width), jnp.bfloat16)
    return local_call(kernel, [*streams, *owns, *arrivals], [shape], name="combine")[0]


def body(
    ring,
    queries,
    keys,
    values,
    proj_weight,
    residual,
    norm_gain,
    route,
    route_weight,
    w_gate,
    w_up,
    w_down,
):
    span = lax.axis_size("sp")
    rows, width = queries.shape[1:]
    heads_here = HEADS // span
    size = width // HEADS
    half = rows // 2
    forward = [(ring[i], ring[(i + 1) % span]) for i in range(span)]
    backward = [(b, a) for a, b in forward]
    mine = [ring.index(position) for position in range(span)]

    shifts = sorted(range(span), key=lambda d: (d > 0, abs(d - span // 2)))
    attended = []
    weights = (w_gate[0], w_up[0], w_down[0])
    for pieces in pack_heads(shifts, queries[0], keys[0], values[0], heads_here, size):
        arrived = [
            lax.ppermute(piece, "sp", [(i, (i + shift) % span) for i in range(span)]) if shift else piece
            for shift, piece in zip(shifts, pieces)
        ]
        result, *loaded = attend(shifts, arrived, size, ())
        attended.append(result)
        weights = loaded or weights

    def projected(offset, part, carried):
        starts = [ring[(spot + offset) % span] * rows + part * half for spot in mine]
        return project_rows(starts, attended, proj_weight, carried, half)

    reach = span // 2
    travelling, message = {}, {}
    for distance in range(reach, 0, -1):
        for first in (1, 0) if distance < reach else (0,):
            for side, pairs in ((1, forward), (-1, backward)):
                part = first if side == 1 else 1 - first
                carried = travelling.get((side, part))
                sent = projected(side * distance, part, carried)
                if first == 1:
                    message[side] = sent
                travelling[side, part] = lax.ppermute(sent, "sp", pairs)

    streams, norms = [], []
    for part in range(2):
        arrivals = [travelling[1, part], travelling[-1, part]]
        stream, normed = finish_rows(
            attended, proj_weight, arrivals, residual[0], norm_gain, route[0], route_weight[0], part
        )
        streams.append(stream)
        norms.append(normed)

    def expert(first, second):
        return expert_pair(first, second, *weights)

    owns = expert(*norms)
    sums = None
    for step in range(1, span):
        norms = [lax.ppermute(n, "sp", p) for n, p in zip(norms, (forward, backward))]
        outs = expert(*norms)
        if sums is not None:
            outs = [a + b for a, b in zip(sums, outs)]
        sums = [lax.ppermute(o, "sp", p) for o, p in zip(outs, (forward, backward))]
    return combine(streams, owns, sums)[None]


def solution(mesh):
    rows = P("dp", "sp", None)
    return jax.shard_map(
        functools.partial(body, ring_order(mesh)),
        mesh=mesh,
        in_specs=(
            rows,
            rows,
            rows,
            P("sp", None),
            rows,
            P(),
            rows,
            rows,
            P("sp", None, None),
            P("sp", None, None),
            P("sp", None, None),
        ),
        out_specs=rows,
        check_vma=False,
    )
```

```python
import functools
import math

import jax
import jax.numpy as jnp
import numpy as np
from jax import lax
from jax.experimental import pallas as pl
from jax.experimental.pallas import tpu as pltpu
from jax.sharding import PartitionSpec as P

HEADS = 16
EPS = 1e-06
VMEM_LIMIT = 16 << 20
EXTRA = 16


def ring_order(mesh, count):
    plain = list(range(count))
    try:
        axis = list(mesh.axis_names).index("sp")
        line = np.moveaxis(mesh.devices, axis, 0)[:count].reshape(count, -1)[:, 0]
        spots = [tuple(device.coords) for device in line]
    except Exception:
        return plain
    moving = [d for d in range(len(spots[0])) if len({s[d] for s in spots}) > 1]
    if len(moving) != 2:
        return plain
    first, second = sorted(moving, key=lambda d: -len({s[d] for s in spots}))
    where = {(s[first], s[second]): i for i, s in enumerate(spots)}
    rows = sorted({s[first] for s in spots})
    cols = sorted({s[second] for s in spots})
    if len(where) != count or len(rows) * len(cols) != count or len(rows) % 2:
        return plain
    path = []
    for number, row in enumerate(rows):
        inner = cols[1:] if number % 2 == 0 else cols[1:][::-1]
        path.extend((row, col) for col in inner)
    path.extend((row, cols[0]) for row in reversed(rows))
    return [where[spot] for spot in path]


def local_call(kernel, operands, shapes, scratch=(), **more):
    vmem = pl.BlockSpec(memory_space=pltpu.VMEM)
    return pl.pallas_call(
        kernel,
        in_specs=[vmem] * len(operands),
        out_specs=[vmem] * len(shapes),
        out_shape=list(shapes),
        scratch_shapes=list(scratch),
        compiler_params=pltpu.CompilerParams(vmem_limit_bytes=VMEM_LIMIT),
        **more,
    )(*operands)


def pack_heads(queries, keys, values, proj_weight, copies_of, span, heads_here, size):
    rows, width = queries.shape
    half_span = span // 2
    group = heads_here * size
    share = proj_weight.shape[0] // copies_of
    tall = half_span

    def kernel(q_ref, k_ref, v_ref, w_ref, *refs):
        near, far = refs[:tall], refs[tall : 2 * tall]
        share_ref, held, arrived = refs[2 * tall :]
        me = lax.axis_index("sp")
        local = lax.rem(me, half_span)
        part_of = pl.multiple_of(lax.axis_index("dp") * share, share)
        copies = [
            pltpu.make_async_copy(source, held.at[part], arrived.at[part])
            for part, source in enumerate((q_ref, k_ref, v_ref))
        ]
        last = pltpu.make_async_copy(w_ref.at[pl.ds(part_of, share), :], share_ref, arrived.at[3])
        for copy in copies:
            copy.start()
        last.start()
        for copy in copies:
            copy.wait()

        def columns(part, owner, head):
            start = pl.multiple_of(owner * group + head * size, size)
            return held[part, :, pl.ds(start, size)]

        for shift in range(half_span):
            target = lax.rem(local + shift, half_span)
            for side in range(2):
                for head in range(heads_here):
                    for part in range(3):
                        to = ((side * heads_here + head) * 3 + part) * size
                        owner = target + side * half_span
                        near[shift][:, to : to + size] = columns(part, owner, head)

        @pl.when(me < half_span)
        def _():
            for shift in range(half_span):
                owner = half_span + lax.rem(local + shift, half_span)
                for head in range(heads_here):
                    for part in range(2):
                        to = (2 * head + part) * size
                        far[shift][:, to : to + size] = columns(1 + part, owner, head)

        @pl.when(me >= half_span)
        def _():
            for shift in range(half_span):
                owner = lax.rem(local + half_span - shift, half_span)
                for head in range(heads_here):
                    for part in range(2):
                        to = (2 * head + part) * size
                        far[shift][:, to : to + size] = columns(0, owner, head)

        last.wait()

    here = [
        pltpu.with_memory_space_constraint(x, pltpu.HBM)
        for x in (queries, keys, values, proj_weight)
    ]
    shapes = [jax.ShapeDtypeStruct((rows, 6 * group), queries.dtype)] * tall
    shapes += [jax.ShapeDtypeStruct((rows, 2 * group), queries.dtype)] * tall
    shapes.append(jax.ShapeDtypeStruct((share, proj_weight.shape[1]), proj_weight.dtype))
    out = pl.pallas_call(
        kernel,
        in_specs=[pl.BlockSpec(memory_space=pltpu.HBM)] * 4,
        out_specs=[pl.BlockSpec(memory_space=pltpu.VMEM)] * len(shapes),
        out_shape=shapes,
        scratch_shapes=[
            pltpu.VMEM((3, rows, width), queries.dtype),
            pltpu.SemaphoreType.DMA((4,)),
        ],
        compiler_params=pltpu.CompilerParams(vmem_limit_bytes=VMEM_LIMIT),
        name="pack_heads",
    )(*here)
    return list(out[:tall]), list(out[tall : 2 * tall]), out[2 * tall]


def stick_breaking(query, key, value, length, size, causal_rows, store):
    block = min(256, length)
    blocks = length // block
    factor = size ** (-0.5) * math.log2(math.e)
    row = lax.broadcasted_iota(jnp.int32, (block, block), 0)
    col = lax.broadcasted_iota(jnp.int32, (block, block), 1)
    later = (row > col).astype(jnp.bfloat16)
    causal = col < row

    def span_of(number):
        return pl.ds(number * block, block)

    def reach(qb):
        return list(range(qb if causal_rows else blocks - 1, -1, -1))

    def scores(qb):
        found = query(span_of(qb))
        return [
            lax.dot_general(
                found,
                key(span_of(kb)),
                (((1,), (1,)), ((), ())),
                preferred_element_type=jnp.float32,
            )
            for kb in reach(qb)
        ]

    def softplus_parts(qb, found):
        parts = []
        for kb, score in zip(reach(qb), found):
            score = score * factor
            soft = jnp.maximum(score, 0.0) + jnp.log2(1.0 + jnp.exp2(-jnp.abs(score)))
            rest = score - soft
            if causal_rows and kb == qb:
                soft = jnp.where(causal, soft, 0.0)
            parts.append((rest, soft.astype(jnp.bfloat16), soft[:, 0:1]))
        return parts

    def finish(qb, parts, sums):
        carry = total = None
        for kb, (rest, _, first), behind in zip(reach(qb), parts, sums):
            power = rest - behind
            if carry is not None:
                power = power - carry
            weight = jnp.exp2(power)
            if causal_rows and kb == qb:
                weight = jnp.where(causal, weight, 0.0)
            part = jnp.dot(
                weight.astype(jnp.bfloat16), value(span_of(kb)), preferred_element_type=jnp.float32
            )
            total = part if total is None else total + part
            passed = behind[:, 0:1] + first
            carry = passed if carry is None else carry + passed
        store(span_of(qb), total, carry)

    found, waiting = scores(0), None
    for qb in range(blocks):
        following = scores(qb + 1) if qb + 1 < blocks else None
        parts = softplus_parts(qb, found)
        sums = [jnp.dot(high, later, preferred_element_type=jnp.float32) for _, high, _ in parts]
        if waiting is not None:
            finish(*waiting)
        waiting, found = (qb, parts, sums), following
    finish(*waiting)


def attend_near(pieces, heads, size):
    rows, columns = pieces[0].shape
    half_span = len(pieces)
    length = rows * half_span

    def kernel(*refs):
        piece_refs, (o_ref, c_ref, x_ref) = refs[:half_span], refs[half_span:]
        local = lax.rem(lax.axis_index("sp"), half_span)
        for shift, piece in enumerate(piece_refs):
            start = pl.multiple_of(lax.rem(local + half_span - shift, half_span) * rows, rows)
            x_ref[pl.ds(start, rows), :] = piece[...]
        lane = lax.broadcasted_iota(jnp.int32, (min(256, length), 128), 1)
        for head in range(heads):
            at = [slice((3 * head + part) * size, (3 * head + part + 1) * size) for part in range(3)]

            def store(where, total, carry, head=head):
                o_ref[where, head * size : (head + 1) * size] = total
                kept = 0.0 if head == 0 else c_ref[where, :]
                c_ref[where, :] = jnp.where(lane == head, carry, kept)

            stick_breaking(
                lambda where: x_ref[where, at[0]],
                lambda where: x_ref[where, at[1]],
                lambda where: x_ref[where, at[2]],
                length,
                size,
                True,
                store,
            )

    return local_call(
        kernel,
        pieces,
        [
            jax.ShapeDtypeStruct((length, heads * size), jnp.float32),
            jax.ShapeDtypeStruct((length, 128), jnp.float32),
        ],
        [pltpu.VMEM((length, columns), pieces[0].dtype)],
        name="attend_near",
    )


def attend_far(near, far, heads, size):
    rows = near[0].shape[0]
    half_span = len(near)
    length = rows * half_span
    group = heads * size

    def kernel(*refs):
        near_refs, far_refs = refs[:half_span], refs[half_span : 2 * half_span]
        o_ref, x_ref = refs[2 * half_span :]
        me = lax.axis_index("sp")
        local = lax.rem(me, half_span)

        def take(ref, place, column, to):
            start = pl.multiple_of(place * rows, rows)
            x_ref[pl.ds(start, rows), to * size : (to + 1) * size] = ref[
                :, column * size : (column + 1) * size
            ]

        @pl.when(me < half_span)
        def _():
            for shift in range(half_span):
                here = lax.rem(local + half_span - shift, half_span)
                there = lax.rem(local + shift, half_span)
                for head in range(heads):
                    take(far_refs[shift], there, 2 * head, 3 * head)
                    for part in (1, 2):
                        take(near_refs[shift], here, 3 * head + part, 3 * head + part)

        @pl.when(me >= half_span)
        def _():
            for shift in range(half_span):
                here = lax.rem(local + half_span - shift, half_span)
                for head in range(heads):
                    take(near_refs[shift], here, 3 * (heads + head), 3 * head)
                    for part in (1, 2):
                        take(far_refs[shift], here, 2 * head + part - 1, 3 * head + part)

        for head in range(heads):
            at = [slice((3 * head + part) * size, (3 * head + part + 1) * size) for part in range(3)]

            def store(where, total, carry, head=head):
                o_ref[where, head * size : (head + 1) * size] = total.astype(o_ref.dtype)

            stick_breaking(
                lambda where: x_ref[where, at[0]],
                lambda where: x_ref[where, at[1]],
                lambda where: x_ref[where, at[2]],
                length,
                size,
                False,
                store,
            )

    return local_call(
        kernel,
        [*near, *far],
        [jax.ShapeDtypeStruct((length, group), near[0].dtype)],
        [pltpu.VMEM((length, 3 * group), near[0].dtype)],
        name="attend_far",
    )[0]


def join_attended(near, sums, sent, own, half_span, heads, size):
    length = near.shape[0]

    def kernel(n_ref, c_ref, s_ref, f_ref, o_ref):
        upper = lax.axis_index("sp") >= half_span

        @pl.when(upper)
        def _():
            for head in range(2 * heads):
                cols = slice(head * size, (head + 1) * size)
                place = head % heads
                ref = s_ref if head < heads else f_ref
                more = ref[:, place * size : (place + 1) * size].astype(jnp.float32)
                fade = jnp.exp2(-c_ref[:, head : head + 1])
                o_ref[:, cols] = (n_ref[:, cols] + fade * more).astype(o_ref.dtype)

        @pl.when(jnp.logical_not(upper))
        def _():
            o_ref[...] = n_ref[...].astype(o_ref.dtype)

    return local_call(
        kernel,
        [near, sums, sent, own],
        [jax.ShapeDtypeStruct((length, near.shape[1]), jnp.bfloat16)],
        name="join_attended",
    )[0]


def join_weights(pieces, labels):
    share, width = pieces[0].shape

    def kernel(*refs):
        replica = lax.axis_index("dp")
        for label, ref in zip(labels, refs):
            start = pl.multiple_of(lax.bitwise_xor(replica, jnp.int32(label)) * share, share)
            refs[-1][pl.ds(start, share), :] = ref[...]

    shape = jax.ShapeDtypeStruct((share * len(pieces), width), pieces[0].dtype)
    return local_call(kernel, pieces, [shape], name="join_weights")[0]


def two_parts(attended_ref, own_ref, other_ref, half_span, where):
    group = own_ref.shape[0]
    upper = (lax.axis_index("sp") >= half_span).astype(jnp.int32)
    total = None
    for ref, place in ((own_ref, upper), (other_ref, 1 - upper)):
        cols = pl.ds(pl.multiple_of(place * group, group), group)
        part = jnp.dot(attended_ref[where, cols], ref[...], preferred_element_type=jnp.float32)
        total = part if total is None else total + part
    return total


def project_rows(starts, attended, own_weight, other_weight, carried, half):
    width = own_weight.shape[1]
    half_span = len(starts)

    def kernel(*refs):
        local = lax.rem(lax.axis_index("sp"), half_span)
        first = jnp.int32(starts[0])
        for position, start in enumerate(starts):
            first = lax.select(local == position, jnp.int32(start), first)
        where = pl.ds(pl.multiple_of(first, half), half)
        total = two_parts(*refs[:3], half_span, where)
        if carried is not None:
            total = total + refs[3][...].astype(jnp.float32)
        refs[-1][...] = total.astype(jnp.bfloat16)

    return local_call(
        kernel,
        [attended, own_weight, other_weight] + ([] if carried is None else [carried]),
        [jax.ShapeDtypeStruct((half, width), jnp.bfloat16)],
        cost_estimate=pl.CostEstimate(
            flops=2 * half * attended.shape[1] * width, transcendentals=0, bytes_accessed=0
        ),
        name="project_rows",
    )[0]


def finish_rows(projected, arrivals, residual, norm_gain, route, route_weight, part, half_span):
    half, width = arrivals[0].shape
    rows = residual.shape[0]

    def kernel(a_ref, w_ref, o_ref, first_ref, second_ref, r_ref, gain_ref, n_ref, s_ref, *outs):
        stream_ref, normed_ref = outs
        mine = slice(part * half, (part + 1) * half)
        local = lax.rem(lax.axis_index("sp"), half_span)
        start = pl.multiple_of(local * rows + part * half, half)
        total = r_ref[mine, :].astype(jnp.float32)
        total = total + first_ref[...].astype(jnp.float32) + second_ref[...].astype(jnp.float32)
        total = total + two_parts(a_ref, w_ref, o_ref, half_span, pl.ds(start, half))
        stream = total.astype(jnp.bfloat16)
        stream_ref[...] = stream
        stream = stream.astype(jnp.float32)
        power = jnp.mean(stream * stream, axis=-1, keepdims=True)
        normed = stream * lax.rsqrt(power + EPS) * gain_ref[...]
        normed = normed.astype(jnp.bfloat16)
        for number in range(width // rows):
            to = slice(number * half, (number + 1) * half)
            normed_ref[to, :] = normed[:, number * rows : (number + 1) * rows]
        lines = []
        for k in range(2):
            lines.append(n_ref[k : k + 1, :].astype(jnp.float32))
            left = s_ref[k : k + 1, :]
            for _ in range(3):
                lines.append(left.astype(jnp.bfloat16).astype(jnp.float32))
                left = left - lines[-1]
        table = jnp.zeros((EXTRA, rows), jnp.float32)
        which = lax.broadcasted_iota(jnp.int32, (EXTRA, rows), 0)
        for number, line in enumerate(lines):
            table = jnp.where(which == number, line, table)
        lane = lax.broadcasted_iota(jnp.int32, (EXTRA, rows), 1)
        table = jnp.where((lane >= half) == bool(part), table, 0.0)
        normed_ref[width // rows * half :, :] = table.astype(jnp.bfloat16)

    return local_call(
        kernel,
        [*projected, *arrivals, residual, norm_gain[None], route.T, route_weight.T],
        [
            jax.ShapeDtypeStruct((half, width), jnp.bfloat16),
            jax.ShapeDtypeStruct((width // rows * half + EXTRA, rows), jnp.bfloat16),
        ],
        name="finish_rows",
    )


def expert_pair(first, second, w_gate, w_up, w_down):
    lanes = first.shape[1]
    rows = lanes // 2
    width, hidden_units = w_gate.shape

    def kernel(a_ref, b_ref, g_ref, u_ref, d_ref, oa_ref, ob_ref, x_ref):
        for part, ref in enumerate((a_ref, b_ref)):
            for number in range(width // lanes):
                cols = slice(number * lanes, (number + 1) * lanes)
                x_ref[part * rows : (part + 1) * rows, cols] = ref[number * rows : (number + 1) * rows, :]
        x = x_ref[...]
        gate = jnp.dot(x, g_ref[...], preferred_element_type=jnp.float32)
        upper = jnp.dot(x, u_ref[...], preferred_element_type=jnp.float32)
        hidden = (gate / (1.0 + jnp.exp(-gate)) * upper).astype(jnp.bfloat16)
        result = jnp.dot(hidden, d_ref[...], preferred_element_type=jnp.float32)
        below = slice(width // lanes * rows, width // lanes * rows + EXTRA)
        info = a_ref[below, :].astype(jnp.float32) + b_ref[below, :].astype(jnp.float32)
        expert = lax.axis_index("sp").astype(jnp.float32)
        line = jnp.zeros((1, lanes), jnp.float32)
        for k in range(2):
            name, high, mid, low = (info[4 * k + j : 4 * k + j + 1, :] for j in range(4))
            line = line + jnp.where(name == expert, (low + mid) + high, 0.0)
        scale = jnp.broadcast_to(line, (lanes, lanes)).T[:, 0:1]
        out = (result * scale).astype(oa_ref.dtype)
        oa_ref[...] = out[:rows]
        ob_ref[...] = out[rows:]

    shape = jax.ShapeDtypeStruct((rows, width), first.dtype)
    return local_call(
        kernel,
        [first, second, w_gate, w_up, w_down],
        [shape, shape],
        [pltpu.VMEM((2 * rows, width), first.dtype)],
        cost_estimate=pl.CostEstimate(
            flops=12 * rows * width * hidden_units,
            transcendentals=2 * rows * hidden_units,
            bytes_accessed=6 * width * hidden_units,
        ),
        name="expert_pair",
    )


def combine(streams, owns, arrivals):
    half, width = streams[0].shape

    def kernel(*refs):
        for part in range(2):
            stream, own, arrived = (refs[2 * j + part][...].astype(jnp.float32) for j in range(3))
            refs[6][part * half : (part + 1) * half, :] = (stream + (arrived + own)).astype(jnp.bfloat16)

    shape = jax.ShapeDtypeStruct((2 * half, width), jnp.bfloat16)
    return local_call(kernel, [*streams, *owns, *arrivals], [shape], name="combine")[0]


def body(
    ring,
    half_ring,
    queries,
    keys,
    values,
    proj_weight,
    residual,
    norm_gain,
    route,
    route_weight,
    w_gate,
    w_up,
    w_down,
):
    span = lax.axis_size("sp")
    rows, width = queries.shape[1:]
    heads_here = HEADS // span
    size = width // HEADS
    half = rows // 2
    forward = [(ring[i], ring[(i + 1) % span]) for i in range(span)]
    backward = [(b, a) for a, b in forward]
    half_span = span // 2
    copies_of = lax.axis_size("dp")
    halves = (0, half_span)

    near, far, share = pack_heads(
        queries[0], keys[0], values[0], proj_weight, copies_of, span, heads_here, size
    )
    for shift in range(half_span):
        pairs = [(i, half_span + (i + shift) % half_span) for i in range(half_span)]
        far[shift] = lax.ppermute(far[shift], "sp", pairs + [(b, a) for a, b in pairs])
    for shift in range(1, half_span):
        pairs = [(base + i, base + (i + shift) % half_span) for base in halves for i in range(half_span)]
        near[shift] = lax.ppermute(near[shift], "sp", pairs)

    other, labels = [lax.ppermute(share, "sp", [(i, (i + half_span) % span) for i in range(span)])], [0]
    near_out, sums = attend_near(near, 2 * heads_here, size)
    far_out = attend_far(near, far, heads_here, size)
    sent = lax.ppermute(far_out, "sp", [(i, i + half_span) for i in range(half_span)])
    other[0], _ = lax.optimization_barrier((other[0], far_out))
    stride = copies_of // 2
    while stride:
        pairs = [(i, i ^ stride) for i in range(copies_of)]
        other = other + [lax.ppermute(piece, "dp", pairs) for piece in other]
        labels = labels + [label ^ stride for label in labels]
        stride //= 2
    other_weight = join_weights(other, labels)

    attended = join_attended(near_out, sums, sent, far_out, half_span, heads_here, size)

    ahead_pairs = [
        (base + half_ring[i], base + half_ring[(i + 1) % half_span])
        for base in halves
        for i in range(half_span)
    ]
    behind_pairs = [(b, a) for a, b in ahead_pairs]
    mine = [half_ring.index(position) for position in range(half_span)]

    def projected(offset, part, carried):
        starts = [half_ring[(spot + offset) % half_span] * rows + part * half for spot in mine]
        return project_rows(starts, attended, proj_weight, other_weight, carried, half)

    reach = half_span // 2
    travelling = {}
    for distance in range(reach, 0, -1):
        for first in (1, 0) if distance < reach else (0,):
            for side, pairs in ((1, ahead_pairs), (-1, behind_pairs)):
                part = first if side == 1 else 1 - first
                message = projected(side * distance, part, travelling.get((side, part)))
                travelling[side, part] = lax.ppermute(message, "sp", pairs)

    streams, norms = [], []
    for part in range(2):
        arrivals = [travelling[1, part], travelling[-1, part]]
        stream, normed = finish_rows(
            (attended, proj_weight, other_weight),
            arrivals,
            residual[0],
            norm_gain,
            route[0],
            route_weight[0],
            part,
            half_span,
        )
        streams.append(stream)
        norms.append(normed)

    weights = (w_gate[0], w_up[0], w_down[0])

    def expert(first, second):
        return expert_pair(first, second, *weights)

    owns = expert(*norms)
    sums = None
    for step in range(1, span):
        norms = [lax.ppermute(n, "sp", p) for n, p in zip(norms, (forward, backward))]
        outs = expert(*norms)
        if sums is not None:
            outs = [a + b for a, b in zip(sums, outs)]
        sums = [lax.ppermute(o, "sp", p) for o, p in zip(outs, (forward, backward))]
    return combine(streams, owns, sums)[None]


def solution(mesh):
    rows = P("dp", "sp", None)
    span = mesh.shape["sp"]
    return jax.shard_map(
        functools.partial(body, ring_order(mesh, span), ring_order(mesh, span // 2)),
        mesh=mesh,
        in_specs=(
            rows,
            rows,
            rows,
            P("sp", None),
            rows,
            P(),
            rows,
            rows,
            P("sp", None, None),
            P("sp", None, None),
            P("sp", None, None),
        ),
        out_specs=rows,
        check_vma=False,
    )
```
